256 devices in a mesh: ep: 16 (over y, x), tp: 16 (over z, core).
Axes of the slice: x: 4, y: 4, z: 8, core: 2. Of those that a mesh axis runs over, the one named last changes fastest.
Arguments:
- tokens: bfloat16 [256, 4096], P('ep'), may hold values from -150 to 150
- query_weight: bfloat16 [4096, 1024], P('tp'), may hold values from -0.09375 to 0.09375
- key_weight: bfloat16 [4096, 1024], P('tp'), may hold values from -0.09375 to 0.09375
- value_weight: bfloat16 [4096, 2048], P(None, 'tp'), may hold values from -0.09375 to 0.09375
- decay_down: bfloat16 [4096, 16], replicated, may hold values from -0.09375 to 0.09375
- decay_up: float32 [16, 1024], replicated, may hold values from -3 to 3
- decay_bias: float32 [1024], replicated, may hold values from -8 to 4
- old_state: float32 [256, 256, 2048], P('ep', None, 'tp'), may hold values from -8 to 8
- out_weight: bfloat16 [2048, 4096], P('tp'), may hold values from -0.1875 to 0.1875
- norm_gain: float32 [4096], replicated, may hold values from 0.2 to 4
- router_weight: bfloat16 [4096, 16], replicated, may hold values from -0.09375 to 0.09375
- routing: int32 [256, 2], P('ep'), may hold values from 0 to 15, all different within a row; in each aligned block of 16 rows (0 to 15, 16 to 31, ...) at most 4 rows name the same one
- glu_weight: bfloat16 [16, 4096, 2048], P('ep', None, 'tp'), may hold values from -0.25 to 0.25
- linear_weight: bfloat16 [16, 4096, 2048], P('ep', None, 'tp'), may hold values from -0.25 to 0.25
- down_weight: bfloat16 [16, 2048, 4096], P('ep', 'tp'), may hold values from -0.01953125 to 0.01953125
- final_gain: float32 [4096], replicated, may hold values from 0.1 to 1.9
Outputs:
- layer_out: bfloat16 [256, 4096], P('ep', 'tp')
- new_state: float32 [256, 256, 2048], P('ep', None, 'tp')
The draws below stay inside these ranges and needn't reach their ends.
Inputs may be any that keep to these rules, and one draw needn't show every extreme that they name: `routing`: within the rows of one device (aligned blocks of 16 rows) no expert is named by more than 4 rows, and at least one block reaches that bound; each row names 2 different experts.
All inputs are finite; a program needn't handle non-finite values.
Results may differ from the reference program's by a relative error of at most 0.015.
Values may be sent and summed in bfloat16 or wider, within the bound.
A program may use at most 64 MiB of HBM per device.

```python
import math
import jax
import jax.numpy as jnp
import numpy as np
from jax import lax

D = 4096
HEADS = 4
HEAD_DK = 256
HEAD_DV = 512
DK = 1024
DV = 2048
RANK = 16
FF = 2048
TOP = 2
SEQ_DEV = 16
SEQS = 256
EXPERTS = 16
CAP = 4


def draw_tokens(key, part):
    row_key, column_key, base_key = jax.random.split(jax.random.fold_in(key, 11), 3)
    position = jnp.arange(D, dtype=jnp.float32) / D
    column = 0.25 * jnp.exp(position * jnp.log(10.0)) * jax.random.uniform(column_key, (D,), jnp.float32, 0.7, 1.3)
    row_scale = jnp.exp(jax.random.uniform(row_key, (SEQS, 1), jnp.float32, -1.15, 1.15))
    base = jnp.clip(jax.random.normal(base_key, (SEQS, D), jnp.float32), -6.0, 6.0)
    return (base * row_scale * column[None, :]).astype(jnp.bfloat16)


def draw_norm_gain(key, part):
    position = jnp.arange(D, dtype=jnp.float32) / D
    rough_key = jax.random.fold_in(key, 23)
    trend = 0.5 * jnp.exp(position * jnp.log(4.0))
    rough = jax.random.uniform(rough_key, (D,), jnp.float32, 0.8, 1.2)
    return (trend * rough).astype(jnp.float32)


def strengthened(values, key, source, target, blocks, factor):
    def block_of(dim):
        return (jnp.arange(values.shape[dim]) // (values.shape[dim] // blocks)).reshape((-1,) + (1,) * (values.ndim - 1 - dim))

    first = jax.random.permutation(key, blocks)[block_of(target)]
    second = (block_of(target) + blocks // 2) % blocks
    return jnp.where((block_of(source) == first) | (block_of(source) == second), factor * values, values)


def shard_levels(key, dims, cuts, least, largest):
    factor_of, own = 1.0, jax.random.fold_in(key, 6)
    for dim, parts in cuts:
        steps = jnp.exp(jax.random.uniform(jax.random.fold_in(own, dim), (parts,), jnp.float32, least / len(cuts), largest / len(cuts)))
        factor_of = factor_of * jnp.repeat(steps, dims[dim] // parts).reshape([-1 if axis == dim else 1 for axis in range(len(dims))])
    return factor_of


def shared_out(rng, own, number, rows, number_of, top, bound, slope):
    ranking = jax.random.permutation(rng, number_of)
    packed, usual = load_shares(number_of, rows * top, bound, slope, True), load_shares(number_of, rows * top, bound, slope, False)
    places = jnp.arange(number_of)

    def named(sizes, rotation):
        used = int((sizes > 0).sum())
        fixed = max(1, used // 4)
        moved = fixed + (places - fixed + rotation * (used - fixed)) % max(1, number_of - fixed)
        return jnp.zeros((number_of,), jnp.int32).at[ranking[jnp.where(places < fixed, places, moved)]].set(jnp.asarray(sizes, jnp.int32))

    sizes = jnp.where(number % 4 == 0, named(packed, number // 4), named(usual, number - number // 4 - 1))
    mixed = jax.random.permutation(jax.random.fold_in(own, 3), number_of)
    source_of, taker = mixed[0:number_of // 2 * 2:2], mixed[1:number_of // 2 * 2:2]
    room = jnp.minimum(sizes[source_of] - 1, bound - sizes[taker]) // 2
    room = jnp.where((source_of == ranking[0]) | (taker == ranking[0]) | (sizes[taker] == 0), 0, jnp.maximum(room, 0))
    moved = jax.random.randint(jax.random.fold_in(own, 4), (number_of // 2,), 0, 1 << 20) % (room + 1)
    sizes = sizes.at[source_of].add(-moved).at[taker].add(moved)
    items = jnp.searchsorted(jnp.cumsum(sizes), jnp.arange(rows * top), side="right").astype(jnp.int32)
    table = items.reshape(top, rows).T
    table = table[jax.random.permutation(jax.random.fold_in(own, 1), rows)]
    rotation = jax.random.randint(jax.random.fold_in(own, 2), (rows, 1), 0, top)
    return jnp.take_along_axis(table, (jnp.arange(top)[None, :] + rotation) % top, axis=1)


def load_shares(number_of, total, limit, lean, full):
    portions = [(1 << 20) // math.isqrt(grade ** lean) + 1 for grade in range(1, number_of + 1)]
    largest = limit if full else min(limit, max(-(-total // number_of), total * portions[0] // sum(portions)))
    least = 1 if total - largest >= number_of - 1 else 0
    given, surplus = [largest] + [least] * (number_of - 1), total - largest - least * (number_of - 1)
    while surplus > 0:
        candidates = [i for i in range(1, number_of) if given[i] < largest] or [i for i in range(1, number_of) if given[i] < limit]
        pool, remaining = sum([portions[i] for i in candidates]), surplus
        for i in candidates:
            extra = min(limit - given[i], max(1, remaining * portions[i] // pool), surplus)
            given[i] = given[i] + extra
            surplus = surplus - extra
    return np.array(given)


def gaussian(key, dims, scale, bound, pieces=(), kind=jnp.bfloat16):
    level = shard_levels(key, dims, pieces, -0.22, 0.18) if pieces else 1.0
    array = jax.random.normal(key, dims, jnp.float32) * scale * level
    return jnp.minimum(jnp.maximum(array, -bound), bound).astype(kind)


def heavy_noise(key, dims, width, bound, cuts, heavy, held_as=jnp.bfloat16):
    array = width * jax.random.normal(key, dims, jnp.float32)
    if cuts:
        array = array * shard_levels(key, dims, cuts, -0.22, 0.18)
    return jnp.clip(strengthened(array, jax.random.fold_in(key, 3), *heavy), -bound, bound).astype(held_as)


def setup_inputs(seed: int = 0) -> dict:
    seeds = jax.random.split(jax.random.key(seed), 17)
    tokens = draw_tokens(jax.random.fold_in(seeds[16], 71), 0)
    query_weight = gaussian(seeds[1], (D, DK), D ** -0.5, 0.09375, ((0, 16),))
    key_weight = gaussian(seeds[2], (D, DK), D ** -0.5, 0.09375, ((0, 16),))
    value_weight = gaussian(seeds[3], (D, DV), D ** -0.5, 0.09375, ((1, 16),))
    decay_down = gaussian(seeds[4], (D, RANK), D ** -0.5, 0.09375)
    decay_up = gaussian(seeds[5], (RANK, DK), (RANK // 4) ** -0.5, 3.0, (), jnp.float32)
    decay_bias = jnp.clip(jax.random.uniform(seeds[6], (DK,), jnp.float32, -8.0, 4.0), -8.0, 4.0)
    old_state = gaussian(seeds[7], (SEQS, HEAD_DK, DV), 2.0, 8.0, ((0, 16), (2, 16)), jnp.float32)
    out_weight = heavy_noise(seeds[8], (DV, D), DV ** -0.5, 0.1875, ((0, 16),), (0, 1, 16, 2.0))
    norm_gain = draw_norm_gain(jax.random.fold_in(seeds[16], 71), 0)
    router_weight = gaussian(seeds[10], (D, EXPERTS), D ** -0.5, 0.09375)
    routing_keys = jax.random.split(jax.random.fold_in(seeds[11], 1), SEQS // SEQ_DEV)
    routing_turns = jax.random.permutation(jax.random.fold_in(seeds[11], 3), SEQS // SEQ_DEV)
    routing = jax.vmap(lambda own, number: shared_out(jax.random.fold_in(seeds[11], 2), own, number, SEQ_DEV, EXPERTS, TOP, CAP, 2))(routing_keys, routing_turns).reshape((SEQS, TOP))
    glu_weight = gaussian(seeds[12], (EXPERTS, D, FF), (D // 9) ** -0.5, 0.25, ((0, 16), (2, 16)))
    linear_weight = gaussian(seeds[13], (EXPERTS, D, FF), (D // 9) ** -0.5, 0.25, ((0, 16), (2, 16)))
    down_weight = heavy_noise(seeds[14], (EXPERTS, FF, D), (FF * 100) ** -0.5, 0.01953125, ((0, 16), (1, 16)), (1, 2, 16, 2.0))
    final_gain = jnp.clip(1.0 + 0.18 * jax.random.normal(seeds[15], (D,), jnp.float32), 0.1, 1.9)
    return {"tokens": tokens, "query_weight": query_weight, "key_weight": key_weight, "value_weight": value_weight, "decay_down": decay_down, "decay_up": decay_up, "decay_bias": decay_bias, "old_state": old_state, "out_weight": out_weight, "norm_gain": norm_gain, "router_weight": router_weight, "routing": routing, "glu_weight": glu_weight, "linear_weight": linear_weight, "down_weight": down_weight, "final_gain": final_gain}


ALPHA = 2.0 ** 0.25
TAU = 16.0
LIMIT = 7.0
SLOPE = 1.702
EPSILON = 1e-05

def layer_norm(inputs, gain):
    mean = lax.optimization_barrier(jnp.mean(inputs, axis=-1, keepdims=True))
    centered = inputs - mean
    variance = lax.optimization_barrier(jnp.mean(centered * centered, axis=-1, keepdims=True))
    return centered * lax.rsqrt(variance + EPSILON) * gain

def clamped_unit(glu_pre, linear_pre):
    glu = jnp.minimum(glu_pre, LIMIT)
    linear = jnp.clip(linear_pre, -LIMIT, LIMIT)
    return glu * jax.nn.sigmoid(SLOPE * glu) * (linear + 1.0)

def reference(tokens, query_weight, key_weight, value_weight, decay_down, decay_up, decay_bias, old_state, out_weight, norm_gain, router_weight, routing, glu_weight, linear_weight, down_weight, final_gain):
    query = jnp.dot(tokens, query_weight, preferred_element_type=jnp.float32).astype(jnp.bfloat16)
    keys = jnp.dot(tokens, key_weight, preferred_element_type=jnp.float32).astype(jnp.bfloat16)
    values = jnp.dot(tokens, value_weight, preferred_element_type=jnp.float32).astype(jnp.bfloat16)
    low_rank = jnp.dot(tokens, decay_down, preferred_element_type=jnp.float32)
    decay = jnp.exp(jax.nn.log_sigmoid(jnp.dot(low_rank, decay_up, precision=lax.Precision.HIGHEST) + decay_bias) / TAU)
    state_parts = []
    mixed_parts = []
    for head in range(HEADS):
        key_cols = slice(head * HEAD_DK, (head + 1) * HEAD_DK)
        value_cols = slice(head * HEAD_DV, (head + 1) * HEAD_DV)
        updated = decay[:, key_cols, None] * old_state[:, :, value_cols] + keys[:, key_cols].astype(jnp.float32)[:, :, None] * values[:, value_cols].astype(jnp.float32)[:, None, :]
        state_parts.append(updated)
        mixed_parts.append(jnp.einsum('bi,bic->bc', query[:, key_cols].astype(jnp.float32), updated, precision=lax.Precision.HIGHEST) * HEAD_DK ** (-0.5))
    new_state = jnp.concatenate(state_parts, axis=2)
    mixed = jnp.concatenate(mixed_parts, axis=1).astype(jnp.bfloat16)
    hidden_in = ALPHA * tokens.astype(jnp.float32) + jnp.dot(mixed, out_weight, preferred_element_type=jnp.float32)
    normed = layer_norm(hidden_in, norm_gain).astype(jnp.bfloat16)
    logits = jnp.dot(normed, router_weight, preferred_element_type=jnp.float32)
    picked = jnp.take_along_axis(logits, routing, axis=1)
    raised = jnp.exp(picked)
    gates = raised / lax.optimization_barrier(jnp.sum(raised, axis=1, keepdims=True))
    expert_ids = jnp.arange(EXPERTS, dtype=jnp.int32)
    chosen = (routing[:, :, None] == expert_ids[None, None, :]).astype(jnp.float32)
    share = lax.optimization_barrier(jnp.sum(chosen * gates[:, :, None], axis=1))

    def one_expert(total, inputs):
        glu_w, linear_w, down_w, column = inputs
        act = clamped_unit(jnp.dot(normed, glu_w, preferred_element_type=jnp.float32), jnp.dot(normed, linear_w, preferred_element_type=jnp.float32)).astype(jnp.bfloat16)
        result = jnp.dot(act, down_w, preferred_element_type=jnp.float32)
        rounded = lax.optimization_barrier((result * column[:, None]).astype(jnp.bfloat16))
        return (total + rounded.astype(jnp.float32), None)
    mixture, _ = lax.scan(one_expert, jnp.zeros((SEQS, D), jnp.float32), (glu_weight, linear_weight, down_weight, share.T))
    combined = ALPHA * normed.astype(jnp.float32) + mixture
    layer_out = layer_norm(combined, final_gain).astype(jnp.bfloat16)
    return (layer_out, new_state)
```

```python
import functools

import jax
import jax.numpy as jnp
from jax import lax
from jax.experimental import pallas as pl
from jax.experimental.pallas import tpu as pltpu
from jax.sharding import PartitionSpec as P

ALPHA = 2.0**0.25
TAU = 16.0
LIMIT = 7.0
SLOPE = 1.702
EPSILON = 1e-05
MESH = pl.DeviceIdType.MESH
F32 = jnp.float32
BF16 = jnp.bfloat16

N = 16
ROWS = 16
D = 4096
PIECE = 256
HALF = 2048
CAP = 4
KEYS = 256
LANES = 128


def dot(a, b):
    return jnp.dot(a, b, preferred_element_type=F32)


def dot_nt(a, b, precision=None):
    return lax.dot_general(a, b, (((1,), (1,)), ((), ())), precision=precision, preferred_element_type=F32)


def iota(shape, dim):
    return lax.broadcasted_iota(jnp.int32, shape, dim)


def remote(src, dst, send_sem, recv_sem, **where):
    return pltpu.make_async_remote_copy(
        src_ref=src, dst_ref=dst, send_sem=send_sem, recv_sem=recv_sem, device_id=where, device_id_type=MESH
    )


def kernel(
    tok_h, qw_h, kw_h, vw_h, dd_h, du_h, db_h, st_h, ow_h, ng_h, rw_h, rt_h, glu_h, lin_h, dn_h, fg_h,
    out_ref, ns_h,
    tok, qw, kw, vw, dd, du, db, st, ow, ng, rw, rt, gl, dn, fg, ns,
    sq, rq, rqk, mixed, sp, rp, rg, h, nrm, sd, rd, rd2, xs, sh, rh, sr, rr, sm, rm, ss, rs,
    loc, s1, r1, s1b, r1b, s2, r2, s3, r3, s4, r4, s4d, r4d, s5, r5, s6, r6, s7, r7, s8, r8,
):
    e = lax.axis_index("ep")
    t = lax.axis_index("tp")
    z = t // 2
    c = lax.rem(t, 2)
    head = t // 4
    member = lax.rem(t, 4)
    partner = t + 1 - 2 * c

    def around(base, step, size):
        return lax.rem(base + step, size)

    head_cols = pl.ds(pl.multiple_of(head * KEYS, KEYS), KEYS)
    fetches = [
        (tok_h, tok), (qw_h, qw), (kw_h, kw), (dd_h, dd), (du_h.at[:, head_cols], du), (db_h.at[:, head_cols], db),
        (vw_h, vw), (st_h, st), (ow_h, ow), (ng_h, ng), (rw_h, rw), (rt_h, rt),
        (glu_h.at[0], gl.at[:, pl.ds(0, LANES)]), (lin_h.at[0], gl.at[:, pl.ds(LANES, LANES)]),
        (dn_h.at[0], dn), (fg_h.at[:, pl.ds(pl.multiple_of(t * PIECE, PIECE), PIECE)], fg),
    ]
    copies = [pltpu.make_async_copy(a, b, loc.at[i]) for i, (a, b) in enumerate(fetches)]
    for copy in copies:
        copy.start()

    def fetched(*which):
        for i in which:
            copies[i].wait()

    barrier = pltpu.get_barrier_semaphore()
    for step in range(1, N):
        pl.semaphore_signal(barrier, inc=1, device_id={"tp": around(t, step, N)}, device_id_type=MESH)
        pl.semaphore_signal(barrier, inc=1, device_id={"ep": around(e, step, N)}, device_id_type=MESH)

    fetched(0, 1, 2)
    share = tok[:, pl.ds(pl.multiple_of(t * PIECE, PIECE), PIECE)]
    q_part = dot(share, qw[...]).astype(BF16)
    k_part = dot(share, kw[...]).astype(BF16)
    for i in range(N):
        part = q_part if i % 4 < 2 else k_part
        at = (i // 4) * KEYS + (i % 2) * LANES
        sq[i] = part[:, at : at + LANES]
    pl.semaphore_wait(barrier, 2 * (N - 1))
    sends = []

    def send(*args, **where):
        copy = remote(*args, **where)
        copy.start()
        sends.append(copy)

    for step in range(1, N):
        to = around(t, step, N)
        send(sq.at[to], rq.at[t], s1.at[to], r1.at[t], tp=to)
    rq[t] = sq[t]

    fetched(3, 4, 5, 6)
    tokens = tok[...]
    values = dot(tokens, vw[...]).astype(BF16)
    low_rank = dot_nt(tokens, dd[...])
    pre = jnp.dot(low_rank, du[...], precision=lax.Precision.HIGHEST, preferred_element_type=F32) + db[...]
    log_sig = -(jnp.maximum(-pre, 0.0) + jnp.log1p(jnp.exp(-jnp.abs(pre))))
    decay = jnp.exp(log_sig / TAU)
    hi = decay.astype(BF16)
    rest = decay - hi.astype(F32)
    mid = rest.astype(BF16)
    low = (rest - mid.astype(F32)).astype(BF16)
    thirds = jnp.concatenate([hi.astype(F32), mid.astype(F32), low.astype(F32)], axis=0)
    wide = ROWS * LANES
    ones3 = (lax.rem(iota((3 * ROWS, wide), 0), ROWS) == iota((3 * ROWS, wide), 1) // LANES).astype(BF16)
    decay_wide = dot(jnp.transpose(thirds).astype(BF16), ones3)
    fetched(7)
    for s in range(ROWS):
        ns[s] = decay_wide[:, s * LANES : (s + 1) * LANES] * st[s]
    own_block = iota((ROWS, wide), 0) == iota((ROWS, wide), 1) // LANES
    ones1 = own_block.astype(BF16)
    values_f = values.astype(F32)
    values_wide = jnp.where(own_block, jnp.concatenate([values_f] * ROWS, axis=1), 0.0).astype(BF16)

    def received(recv, sems, step, base, size, axis):
        src = around(base, step, size)
        remote(recv.at[src], recv.at[src], s1.at[0], sems.at[src], **{axis: src}).wait_recv()

    for step in range(1, N):
        received(rq, r1, step, t, N, "tp")
    rqk[member] = jnp.sum(rq[...].astype(F32), axis=0).astype(BF16)
    for step in range(1, 4):
        to = around(member, step, 4)
        send(rqk.at[member], rqk.at[member], s1b.at[to], r1b.at[member], tp=head * 4 + to)
    for step in range(1, 4):
        src = around(member, step, 4)
        remote(rqk.at[src], rqk.at[src], s1b.at[0], r1b.at[src], tp=head * 4 + src).wait_recv()

    query = jnp.concatenate([rqk[0], rqk[1]], axis=1).astype(F32)
    keys = jnp.concatenate([rqk[2], rqk[3]], axis=1).astype(F32)
    update = dot(jnp.transpose(keys).astype(BF16), values_wide)
    query_wide = dot(jnp.transpose(query).astype(BF16), ones1)
    for s in range(ROWS):
        cols = slice(s * LANES, (s + 1) * LANES)
        new = ns[s] + update[:, cols]
        ns[s] = new
        mixed[s : s + 1, :] = jnp.sum(query_wide[:, cols] * new, axis=0, keepdims=True)
    state_out = pltpu.make_async_copy(ns, ns_h, loc.at[16])
    state_out.start()

    fetched(8)
    attn_part = dot((mixed[...] * KEYS ** (-0.5)).astype(BF16), ow[...]).astype(BF16)
    for i in range(N):
        sp[i] = attn_part[:, i * PIECE : (i + 1) * PIECE]
    for step in range(1, N):
        to = around(t, step, N)
        send(sp.at[to], rp.at[t], s2.at[to], r2.at[t], tp=to)
    rp[t] = sp[t]

    fetched(9, 10, 11)
    slots = N * CAP
    routed = rt[...]
    ids = iota((N, ROWS), 0)
    chosen = ((routed[0:1, :] == ids) | (routed[1:2, :] == ids)).astype(F32)
    upper = (iota((ROWS, ROWS), 0) < iota((ROWS, ROWS), 1)).astype(BF16)
    rank = dot(chosen.astype(BF16), upper)
    expand = (iota((slots, N), 0) // CAP == iota((slots, N), 1)).astype(BF16)
    here = dot(expand, chosen.astype(BF16)) > 0.5
    place = dot(expand, rank.astype(BF16))
    spread = (here & (place == lax.rem(iota((slots, ROWS), 0), CAP).astype(F32))).astype(F32)

    for step in range(1, N):
        received(rp, r2, step, t, N, "tp")
    rg[t] = jnp.sum(rp[...].astype(F32), axis=0).astype(BF16)
    for step in range(1, N):
        to = around(t, step, N)
        send(rg.at[t], rg.at[t], s3.at[to], r3.at[t], tp=to)
    for step in range(1, N):
        received(rg, r3, step, t, N, "tp")

    for i in range(N):
        cols = slice(i * PIECE, (i + 1) * PIECE)
        h[:, cols] = ALPHA * tok[:, cols].astype(F32) + rg[i].astype(F32)
    hidden = h[...]
    centred = hidden - jnp.mean(hidden, axis=1, keepdims=True)
    var = jnp.mean(centred * centred, axis=1, keepdims=True)
    nrm[...] = (centred * lax.rsqrt(var + EPSILON) * ng[...]).astype(BF16)

    def block(j, core):
        return pl.ds(pl.multiple_of((2 * j + core) * PIECE, PIECE), PIECE)

    half = jnp.concatenate([nrm[:, block(j, c)] for j in range(N // 2)], axis=1)
    packed = dot(spread.astype(BF16), half)
    for i in range(N):
        sd[i] = packed[i * CAP : (i + 1) * CAP].astype(BF16)
    for step in range(1, N):
        to = around(e, step, N)
        send(sd.at[to], rd.at[e], s4.at[to], r4.at[e], ep=to)
    send(sd.at[e], rd2.at[e], s4d.at[e], r4d.at[e], tp=partner)
    rd[e] = sd[e]

    logits = dot_nt(rw[...], nrm[...])
    raised = jnp.where(chosen > 0.5, jnp.exp(logits), 0.0)
    gates = raised / jnp.sum(raised, axis=0, keepdims=True)
    gate_rows = spread * jnp.dot(
        expand.astype(F32), gates, precision=lax.Precision.HIGHEST, preferred_element_type=F32
    )
    gate_cols = jnp.transpose(gate_rows)
    gate_hi = gate_cols.astype(BF16)
    gate_lo = (gate_cols - gate_hi.astype(F32)).astype(BF16)

    for step in range(1, N):
        received(rd, r4, step, e, N, "ep")
        src = around(e, step, N)
        send(rd.at[src], rd2.at[src], s4d.at[src], r4d.at[src], tp=partner)
    fetched(12, 13)
    for i in range(N):
        xs[i * CAP : (i + 1) * CAP, :] = rd[i].astype(F32)
    rows = xs[...].astype(BF16)
    pre_act = sum(dot(rows[:, j * PIECE : (j + 1) * PIECE], gl[block(j, c), :]) for j in range(N // 2))
    for i in range(N):
        remote(rd2.at[i], rd2.at[i], s1.at[0], r4d.at[i], tp=partner).wait_recv()
    for i in range(N):
        xs[i * CAP : (i + 1) * CAP, :] = rd2[i].astype(F32)
    rows = xs[...].astype(BF16)
    pre_act += sum(dot(rows[:, j * PIECE : (j + 1) * PIECE], gl[block(j, 1 - c), :]) for j in range(N // 2))
    glu = jnp.minimum(pre_act[:, :LANES], LIMIT)
    linear = jnp.clip(pre_act[:, LANES:], -LIMIT, LIMIT)
    act = (glu * jax.nn.sigmoid(SLOPE * glu) * (linear + 1.0)).astype(BF16)

    fetched(14)
    for j in range(N // 2):
        sh[j] = dot(act, dn[:, block(j, 1 - c)]).astype(BF16)
        send(sh.at[j], rh.at[j], s5.at[j], r5.at[j], tp=partner)
    for j in range(N // 2):
        mine = dot(act, dn[:, block(j, c)])
        remote(rh.at[j], rh.at[j], s1.at[0], r5.at[j], tp=partner).wait_recv()
        total = (mine + rh[j].astype(F32)).astype(BF16)
        for i in range(N):
            sr[i, :, j * PIECE : (j + 1) * PIECE] = total[i * CAP : (i + 1) * CAP]
    for step in range(1, N):
        to = around(e, step, N)
        send(sr.at[to], rr.at[e], s6.at[to], r6.at[e], ep=to)
    rr[e] = sr[e]
    for step in range(1, N):
        received(rr, r6, step, e, N, "ep")

    for i in range(N):
        xs[i * CAP : (i + 1) * CAP, :] = rr[i].astype(F32)
    back = xs[...].astype(BF16)
    mix = (dot(gate_hi, back) + dot(gate_lo, back)).astype(BF16)
    for j in range(N // 2):
        sm[j] = mix[:, j * PIECE : (j + 1) * PIECE]
    for step in range(1, N // 2):
        to = around(z, step, N // 2)
        send(sm.at[to], rm.at[z], s7.at[to], r7.at[z], tp=2 * to + c)
    rm[z] = sm[z]
    for step in range(1, N // 2):
        src = around(z, step, N // 2)
        remote(rm.at[src], rm.at[src], s1.at[0], r7.at[src], tp=2 * src + c).wait_recv()
    own = nrm[:, pl.ds(pl.multiple_of(t * PIECE, PIECE), PIECE)].astype(F32)
    u = ALPHA * own + jnp.sum(rm[...].astype(F32), axis=0)

    part_mean = jnp.mean(u, axis=1, keepdims=True)
    part_sq = jnp.sum((u - part_mean) ** 2, axis=1, keepdims=True)
    lane, row = iota((ROWS, LANES), 1), iota((ROWS, LANES), 0)
    line = jnp.where(lane == row, part_mean, jnp.where(lane == row + ROWS, part_sq, 0.0))
    ss[...] = jnp.sum(line, axis=0, keepdims=True)
    for step in range(1, N):
        to = around(t, step, N)
        send(ss, rs.at[t], s8.at[to], r8.at[t], tp=to)
    rs[t] = ss[...]
    fetched(15)
    for step in range(1, N):
        received(rs, r8, step, t, N, "tp")
    means = jnp.concatenate([rs[i] for i in range(N)], axis=0)
    total = jnp.sum(means, axis=0, keepdims=True)
    spread_sq = jnp.sum((means - total / N) ** 2, axis=0, keepdims=True)
    mean = jnp.sum(jnp.where(lane == row, total / N, 0.0), axis=1, keepdims=True)
    between = jnp.sum(jnp.where(lane == row, spread_sq, 0.0), axis=1, keepdims=True)
    within = jnp.sum(jnp.where(lane == row + ROWS, total, 0.0), axis=1, keepdims=True)
    variance = (within + PIECE * between) / D
    out_ref[...] = ((u - mean) * lax.rsqrt(variance + EPSILON) * fg[...]).astype(BF16)

    state_out.wait()
    for copy in sends:
        copy.wait_send()


def step(
    tokens, query_weight, key_weight, value_weight, decay_down, decay_up, decay_bias, old_state, out_weight,
    norm_gain, router_weight, routing, glu_weight, linear_weight, down_weight, final_gain,
):
    hbm = pl.BlockSpec(memory_space=pl.ANY)
    vmem, dma = pltpu.VMEM, pltpu.SemaphoreType.DMA
    return pl.pallas_call(
        kernel,
        out_shape=(
            jax.ShapeDtypeStruct((ROWS, PIECE), BF16),
            jax.ShapeDtypeStruct(old_state.shape, F32),
        ),
        in_specs=[hbm] * 16,
        out_specs=(pl.BlockSpec(memory_space=pltpu.VMEM), hbm),
        scratch_shapes=[
            vmem((ROWS, D), BF16), vmem((PIECE, 1024), BF16), vmem((PIECE, 1024), BF16), vmem((D, LANES), BF16),
            vmem((N, D), BF16), vmem((16, KEYS), F32), vmem((1, KEYS), F32), vmem((ROWS, KEYS, LANES), F32),
            vmem((LANES, D), BF16), vmem((1, D), F32), vmem((N, D), BF16), vmem((2, ROWS), jnp.int32),
            vmem((D, 2 * LANES), BF16), vmem((LANES, D), BF16), vmem((1, PIECE), F32), vmem((ROWS, KEYS, LANES), F32),
            vmem((N, ROWS, LANES), BF16), vmem((N, ROWS, LANES), BF16), vmem((4, ROWS, LANES), BF16),
            vmem((ROWS, LANES), F32), vmem((N, ROWS, PIECE), BF16), vmem((N, ROWS, PIECE), BF16),
            vmem((N, ROWS, PIECE), BF16), vmem((ROWS, D), F32), vmem((ROWS, D), BF16),
            vmem((N, CAP, HALF), BF16), vmem((N, CAP, HALF), BF16), vmem((N, CAP, HALF), BF16),
            vmem((N * CAP, HALF), F32), vmem((N // 2, N * CAP, PIECE), BF16), vmem((N // 2, N * CAP, PIECE), BF16),
            vmem((N, CAP, HALF), BF16), vmem((N, CAP, HALF), BF16), vmem((N // 2, ROWS, PIECE), BF16),
            vmem((N // 2, ROWS, PIECE), BF16), vmem((1, LANES), F32), vmem((N, 1, LANES), F32),
            dma((17,)), dma((N,)), dma((N,)), dma((4,)), dma((4,)), dma((N,)), dma((N,)), dma((N,)), dma((N,)),
            dma((N,)), dma((N,)), dma((N,)), dma((N,)), dma((N // 2,)), dma((N // 2,)), dma((N,)), dma((N,)),
            dma((N // 2,)), dma((N // 2,)), dma((N,)), dma((N,)),
        ],
        compiler_params=pltpu.CompilerParams(
            collective_id=0, has_side_effects=True, vmem_limit_bytes=60 * 1024 * 1024
        ),
        name="decode_step",
    )(
        tokens, query_weight, key_weight, value_weight, decay_down.T, decay_up, decay_bias.reshape(1, -1), old_state,
        out_weight, norm_gain.reshape(1, -1), router_weight.T, routing.T, glu_weight, linear_weight, down_weight,
        final_gain.reshape(1, -1),
    )


def solution(mesh):
    in_specs = (
        P("ep", None), P("tp", None), P("tp", None), P(None, "tp"), P(), P(), P(), P("ep", None, "tp"), P("tp", None),
        P(), P(), P("ep", None), P("ep", None, "tp"), P("ep", None, "tp"), P("ep", "tp", None), P(),
    )
    out_specs = (P("ep", "tp"), P("ep", None, "tp"))
    return jax.shard_map(step, mesh=mesh, in_specs=in_specs, out_specs=out_specs, check_vma=False)
```

```python
import functools

import jax
import jax.numpy as jnp
from jax import lax
from jax.experimental import pallas as pl
from jax.experimental.pallas import tpu as pltpu
from jax.sharding import PartitionSpec as P

ALPHA = 2.0**0.25
TAU = 16.0
LIMIT = 7.0
SLOPE = 1.702
EPSILON = 1e-05
MESH = pl.DeviceIdType.MESH
F32 = jnp.float32
BF16 = jnp.bfloat16

N = 16
ROWS = 16
D = 4096
PIECE = 256
HALF = 2048
CAP = 4
KEYS = 256
LANES = 128


def dot(a, b):
    return jnp.dot(a, b, preferred_element_type=F32)


def dot_nt(a, b, precision=None):
    return lax.dot_general(a, b, (((1,), (1,)), ((), ())), precision=precision, preferred_element_type=F32)


def iota(shape, dim):
    return lax.broadcasted_iota(jnp.int32, shape, dim)


_scopes = []


def mark(name):
    while _scopes:
        _scopes.pop().__exit__(None, None, None)
    if name:
        _scopes.append(jax.named_scope(name))
        _scopes[-1].__enter__()


def remote(src, dst, send_sem, recv_sem, **where):
    return pltpu.make_async_remote_copy(
        src_ref=src, dst_ref=dst, send_sem=send_sem, recv_sem=recv_sem, device_id=where, device_id_type=MESH
    )


def kernel(
    tok_h, qw_h, kw_h, vw_h, dd_h, du_h, db_h, st_h, ow_h, ng_h, rw_h, rt_h, glu_h, lin_h, dn_h, fg_h,
    out_ref, ns,
    tok, qw, kw, vw, dd, du, db, st, ow, ng, rw, rt, gl, dn, fg,
    sq, rq, rqk, mixed, sp, rp, rg, h, nrm, sd, rd, rd2, xs, sh, rh, sr, rr, sm, rm, ss, rs,
    loc, out_sem, in_sem,
):
    e = lax.axis_index("ep")
    t = lax.axis_index("tp")
    z = t // 2
    c = lax.rem(t, 2)
    head = t // 4
    member = lax.rem(t, 4)
    partner = t + 1 - 2 * c

    def around(base, step, size):
        return lax.rem(base + step, size)

    mark("fetch")
    head_cols = pl.ds(pl.multiple_of(head * KEYS, KEYS), KEYS)
    fetches = [
        (tok_h, tok), (qw_h, qw), (kw_h, kw), (dd_h, dd), (du_h.at[:, head_cols], du), (db_h.at[:, head_cols], db),
        (vw_h, vw), (st_h, st), (ow_h, ow), (ng_h, ng), (rw_h, rw), (rt_h, rt),
        (glu_h.at[0], gl.at[:, pl.ds(0, LANES)]), (lin_h.at[0], gl.at[:, pl.ds(LANES, LANES)]),
        (dn_h.at[0], dn), (fg_h.at[:, pl.ds(pl.multiple_of(t * PIECE, PIECE), PIECE)], fg),
    ]
    copies = [pltpu.make_async_copy(a, b, loc.at[i]) for i, (a, b) in enumerate(fetches)]
    for copy in copies:
        copy.start()

    def fetched(*which):
        for i in which:
            copies[i].wait()

    mark("barrier_signal")
    barrier = pltpu.get_barrier_semaphore()
    for step in range(1, N):
        pl.semaphore_signal(barrier, inc=1, device_id={"tp": around(t, step, N)}, device_id_type=MESH)
        pl.semaphore_signal(barrier, inc=1, device_id={"ep": around(e, step, N)}, device_id_type=MESH)

    mark("qk_fetch_wait")
    fetched(0, 1, 2)
    mark("qk_dot")
    share = tok[:, pl.ds(pl.multiple_of(t * PIECE, PIECE), PIECE)]
    q_part = dot(share, qw[...]).astype(BF16)
    k_part = dot(share, kw[...]).astype(BF16)
    for i in range(N):
        part = q_part if i % 4 < 2 else k_part
        at = (i // 4) * KEYS + (i % 2) * LANES
        sq[i] = part[:, at : at + LANES]
    mark("barrier_wait")
    pl.semaphore_wait(barrier, 2 * (N - 1))
    mark("s1_send")
    pending = []

    def send(phase, src, dst, **where):
        remote(src, dst, out_sem.at[phase], in_sem.at[phase], **where).start()

    def sent(phase, like, count):
        pending.append((phase, like, count))

    def whole(phase, like, count):
        ref = like if count is None else like.at[pl.ds(0, count)]
        return remote(ref, ref, out_sem.at[phase], in_sem.at[phase], tp=partner)

    def arrived(phase, like, count):
        whole(phase, like, count).wait_recv()

    for step in range(1, N):
        to = around(t, step, N)
        send(0, sq.at[to], rq.at[t], tp=to)
    sent(0, sq, N - 1)
    rq[t] = sq[t]

    mark("decay")
    fetched(3, 4, 5, 6)
    tokens = tok[...]
    values = dot(tokens, vw[...]).astype(BF16)
    low_rank = dot_nt(tokens, dd[...])
    pre = jnp.dot(low_rank, du[...], precision=lax.Precision.HIGHEST, preferred_element_type=F32) + db[...]
    log_sig = -(jnp.maximum(-pre, 0.0) + jnp.log1p(jnp.exp(-jnp.abs(pre))))
    decay = jnp.exp(log_sig / TAU)
    hi = decay.astype(BF16)
    rest = decay - hi.astype(F32)
    mid = rest.astype(BF16)
    low = (rest - mid.astype(F32)).astype(BF16)
    thirds = jnp.concatenate([hi.astype(F32), mid.astype(F32), low.astype(F32)], axis=0)
    wide = ROWS * LANES
    ones3 = (lax.rem(iota((3 * ROWS, wide), 0), ROWS) == iota((3 * ROWS, wide), 1) // LANES).astype(BF16)
    decay_wide = dot(jnp.transpose(thirds).astype(BF16), ones3)
    mark("state_decay")
    fetched(7)
    for s in range(ROWS):
        ns[s] = decay_wide[:, s * LANES : (s + 1) * LANES] * st[s]
    own_block = iota((ROWS, wide), 0) == iota((ROWS, wide), 1) // LANES
    ones1 = own_block.astype(BF16)
    values_f = values.astype(F32)
    values_wide = jnp.where(own_block, jnp.concatenate([values_f] * ROWS, axis=1), 0.0).astype(BF16)

    mark("r1_wait")
    arrived(0, rq, N - 1)
    mark("r1_sum_r1b")
    rqk[member] = jnp.sum(rq[...].astype(F32), axis=0).astype(BF16)
    for step in range(1, 4):
        to = around(member, step, 4)
        send(1, rqk.at[member], rqk.at[member], tp=head * 4 + to)
    sent(1, rqk, 3)
    arrived(1, rqk, 3)

    mark("state")
    query = jnp.concatenate([rqk[0], rqk[1]], axis=1).astype(F32)
    keys = jnp.concatenate([rqk[2], rqk[3]], axis=1).astype(F32)
    update = dot(jnp.transpose(keys).astype(BF16), values_wide)
    query_wide = dot(jnp.transpose(query).astype(BF16), ones1)
    for s in range(ROWS):
        cols = slice(s * LANES, (s + 1) * LANES)
        new = ns[s] + update[:, cols]
        ns[s] = new
        mixed[s : s + 1, :] = jnp.sum(query_wide[:, cols] * new, axis=0, keepdims=True)

    mark("out_dot_s2")
    fetched(8)
    attn_part = dot((mixed[...] * KEYS ** (-0.5)).astype(BF16), ow[...]).astype(BF16)
    for i in range(N):
        sp[i] = attn_part[:, i * PIECE : (i + 1) * PIECE]
    for step in range(1, N):
        to = around(t, step, N)
        send(2, sp.at[to], rp.at[t], tp=to)
    sent(2, sp, N - 1)
    rp[t] = sp[t]

    mark("slots")
    fetched(9, 10, 11)
    slots = N * CAP
    routed = rt[...]
    ids = iota((N, ROWS), 0)
    chosen = ((routed[0:1, :] == ids) | (routed[1:2, :] == ids)).astype(F32)
    upper = (iota((ROWS, ROWS), 0) < iota((ROWS, ROWS), 1)).astype(BF16)
    rank = dot(chosen.astype(BF16), upper)
    expand = (iota((slots, N), 0) // CAP == iota((slots, N), 1)).astype(BF16)
    here = dot(expand, chosen.astype(BF16)) > 0.5
    place = dot(expand, rank.astype(BF16))
    spread = (here & (place == lax.rem(iota((slots, ROWS), 0), CAP).astype(F32))).astype(F32)

    mark("r2_wait")
    arrived(2, rp, N - 1)
    mark("s3_send")
    rg[t] = jnp.sum(rp[...].astype(F32), axis=0).astype(BF16)
    for step in range(1, N):
        to = around(t, step, N)
        send(3, rg.at[t], rg.at[t], tp=to)
    sent(3, rg, N - 1)
    mark("r3_wait")
    arrived(3, rg, N - 1)

    mark("norm1")
    for i in range(N):
        cols = slice(i * PIECE, (i + 1) * PIECE)
        h[:, cols] = ALPHA * tok[:, cols].astype(F32) + rg[i].astype(F32)
    hidden = h[...]
    centred = hidden - jnp.mean(hidden, axis=1, keepdims=True)
    var = jnp.mean(centred * centred, axis=1, keepdims=True)
    nrm[...] = (centred * lax.rsqrt(var + EPSILON) * ng[...]).astype(BF16)

    def block(j, core):
        return pl.ds(pl.multiple_of((2 * j + core) * PIECE, PIECE), PIECE)

    mark("s4_send")
    half = jnp.concatenate([nrm[:, block(j, c)] for j in range(N // 2)], axis=1)
    packed = dot(spread.astype(BF16), half)
    for i in range(N):
        sd[i] = packed[i * CAP : (i + 1) * CAP].astype(BF16)
    for step in range(1, N):
        to = around(e, step, N)
        send(4, sd.at[to], rd.at[e], ep=to)
    sent(4, sd, N - 1)
    send(5, sd.at[e], rd2.at[e], tp=partner)
    sent(5, sd, 1)
    rd[e] = sd[e]

    mark("gates")
    logits = dot_nt(rw[...], nrm[...])
    raised = jnp.where(chosen > 0.5, jnp.exp(logits), 0.0)
    gates = raised / jnp.sum(raised, axis=0, keepdims=True)
    gate_rows = spread * jnp.dot(
        expand.astype(F32), gates, precision=lax.Precision.HIGHEST, preferred_element_type=F32
    )
    gate_cols = jnp.transpose(gate_rows)
    gate_hi = gate_cols.astype(BF16)
    gate_lo = (gate_cols - gate_hi.astype(F32)).astype(BF16)

    mark("r4_wait_fwd")
    arrived(4, rd, N - 1)
    for step in range(1, N):
        src = around(e, step, N)
        send(6, rd.at[src], rd2.at[src], tp=partner)
    sent(6, rd, N - 1)
    mark("up_own")
    fetched(12, 13)
    for i in range(N):
        xs[i * CAP : (i + 1) * CAP, :] = rd[i].astype(F32)
    rows = xs[...].astype(BF16)
    pre_act = sum(dot(rows[:, j * PIECE : (j + 1) * PIECE], gl[block(j, c), :]) for j in range(N // 2))
    mark("r4d_wait")
    arrived(5, rd2, 1)
    arrived(6, rd2, N - 1)
    mark("up_other")
    for i in range(N):
        xs[i * CAP : (i + 1) * CAP, :] = rd2[i].astype(F32)
    rows = xs[...].astype(BF16)
    pre_act += sum(dot(rows[:, j * PIECE : (j + 1) * PIECE], gl[block(j, 1 - c), :]) for j in range(N // 2))
    glu = jnp.minimum(pre_act[:, :LANES], LIMIT)
    linear = jnp.clip(pre_act[:, LANES:], -LIMIT, LIMIT)
    act = (glu * jax.nn.sigmoid(SLOPE * glu) * (linear + 1.0)).astype(BF16)

    mark("down")
    fetched(14)
    for j in range(N // 2):
        sh[j] = dot(act, dn[:, block(j, 1 - c)]).astype(BF16)
        send(7, sh.at[j], rh.at[j], tp=partner)
    sent(7, sh, None)
    mine = [dot(act, dn[:, block(j, c)]) for j in range(N // 2)]
    mark("down_wait")
    arrived(7, rh, None)
    mark("down_sum")
    for j in range(N // 2):
        total = (mine[j] + rh[j].astype(F32)).astype(BF16)
        for i in range(N):
            sr[i, :, j * PIECE : (j + 1) * PIECE] = total[i * CAP : (i + 1) * CAP]
    mark("s6_send")
    for step in range(1, N):
        to = around(e, step, N)
        send(8, sr.at[to], rr.at[e], ep=to)
    sent(8, sr, N - 1)
    rr[e] = sr[e]
    mark("r6_wait")
    arrived(8, rr, N - 1)

    mark("mix_s7")
    for i in range(N):
        xs[i * CAP : (i + 1) * CAP, :] = rr[i].astype(F32)
    back = xs[...].astype(BF16)
    mix = (dot(gate_hi, back) + dot(gate_lo, back)).astype(BF16)
    for j in range(N // 2):
        sm[j] = mix[:, j * PIECE : (j + 1) * PIECE]
    for step in range(1, N // 2):
        to = around(z, step, N // 2)
        send(9, sm.at[to], rm.at[z], tp=2 * to + c)
    sent(9, sm, N // 2 - 1)
    rm[z] = sm[z]
    mark("r7_wait")
    arrived(9, rm, N // 2 - 1)
    mark("stats_s8")
    own = nrm[:, pl.ds(pl.multiple_of(t * PIECE, PIECE), PIECE)].astype(F32)
    u = ALPHA * own + jnp.sum(rm[...].astype(F32), axis=0)

    part_mean = jnp.mean(u, axis=1, keepdims=True)
    part_sq = jnp.sum((u - part_mean) ** 2, axis=1, keepdims=True)
    lane, row = iota((ROWS, LANES), 1), iota((ROWS, LANES), 0)
    line = jnp.where(lane == row, part_mean, jnp.where(lane == row + ROWS, part_sq, 0.0))
    ss[...] = jnp.sum(line, axis=0, keepdims=True)
    for step in range(1, N):
        to = around(t, step, N)
        send(10, ss, rs.at[t], tp=to)
    sent(10, rs, N - 1)
    rs[t] = ss[...]
    mark("r8_wait")
    fetched(15)
    arrived(10, rs, N - 1)
    mark("final")
    means = jnp.concatenate([rs[i] for i in range(N)], axis=0)
    total = jnp.sum(means, axis=0, keepdims=True)
    spread_sq = jnp.sum((means - total / N) ** 2, axis=0, keepdims=True)
    mean = jnp.sum(jnp.where(lane == row, total / N, 0.0), axis=1, keepdims=True)
    between = jnp.sum(jnp.where(lane == row, spread_sq, 0.0), axis=1, keepdims=True)
    within = jnp.sum(jnp.where(lane == row + ROWS, total, 0.0), axis=1, keepdims=True)
    variance = (within + PIECE * between) / D
    out_ref[...] = ((u - mean) * lax.rsqrt(variance + EPSILON) * fg[...]).astype(BF16)

    mark("drain")
    for phase, like, count in pending:
        whole(phase, like, count).wait_send()
    mark(None)


def step(
    tokens, query_weight, key_weight, value_weight, decay_down, decay_up, decay_bias, old_state, out_weight,
    norm_gain, router_weight, routing, glu_weight, linear_weight, down_weight, final_gain,
):
    hbm = pl.BlockSpec(memory_space=pl.ANY)
    vmem, dma = pltpu.VMEM, pltpu.SemaphoreType.DMA
    return pl.pallas_call(
        kernel,
        out_shape=(
            pltpu.VMEM((ROWS, PIECE), BF16),
            pltpu.VMEM(old_state.shape, F32),
        ),
        in_specs=[hbm] * 16,
        out_specs=(pl.BlockSpec(memory_space=pltpu.VMEM), pl.BlockSpec(memory_space=pltpu.VMEM)),
        scratch_shapes=[
            vmem((ROWS, D), BF16), vmem((PIECE, 1024), BF16), vmem((PIECE, 1024), BF16), vmem((D, LANES), BF16),
            vmem((N, D), BF16), vmem((16, KEYS), F32), vmem((1, KEYS), F32), vmem((ROWS, KEYS, LANES), F32),
            vmem((LANES, D), BF16), vmem((1, D), F32), vmem((N, D), BF16), vmem((2, ROWS), jnp.int32),
            vmem((D, 2 * LANES), BF16), vmem((LANES, D), BF16), vmem((1, PIECE), F32),
            vmem((N, ROWS, LANES), BF16), vmem((N, ROWS, LANES), BF16), vmem((4, ROWS, LANES), BF16),
            vmem((ROWS, LANES), F32), vmem((N, ROWS, PIECE), BF16), vmem((N, ROWS, PIECE), BF16),
            vmem((N, ROWS, PIECE), BF16), vmem((ROWS, D), F32), vmem((ROWS, D), BF16),
            vmem((N, CAP, HALF), BF16), vmem((N, CAP, HALF), BF16), vmem((N, CAP, HALF), BF16),
            vmem((N * CAP, HALF), F32), vmem((N // 2, N * CAP, PIECE), BF16), vmem((N // 2, N * CAP, PIECE), BF16),
            vmem((N, CAP, HALF), BF16), vmem((N, CAP, HALF), BF16), vmem((N // 2, ROWS, PIECE), BF16),
            vmem((N // 2, ROWS, PIECE), BF16), vmem((1, LANES), F32), vmem((N, 1, LANES), F32),
            dma((16,)), dma((11,)), dma((11,)),
        ],
        compiler_params=pltpu.CompilerParams(
            collective_id=0, has_side_effects=True, vmem_limit_bytes=60 * 1024 * 1024
        ),
        name="decode_step",
    )(
        tokens, query_weight, key_weight, value_weight, decay_down.T, decay_up, decay_bias.reshape(1, -1), old_state,
        out_weight, norm_gain.reshape(1, -1), router_weight.T, routing.T, glu_weight, linear_weight, down_weight,
        final_gain.reshape(1, -1),
    )


def solution(mesh):
    in_specs = (
        P("ep", None), P("tp", None), P("tp", None), P(None, "tp"), P(), P(), P(), P("ep", None, "tp"), P("tp", None),
        P(), P(), P("ep", None), P("ep", None, "tp"), P("ep", None, "tp"), P("ep", "tp", None), P(),
    )
    out_specs = (P("ep", "tp"), P("ep", None, "tp"))
    return jax.shard_map(step, mesh=mesh, in_specs=in_specs, out_specs=out_specs, check_vma=False)
```

```python
import functools

import jax
import jax.numpy as jnp
from jax import lax
from jax.experimental import pallas as pl
from jax.experimental.pallas import tpu as pltpu
from jax.sharding import PartitionSpec as P

ALPHA = 2.0**0.25
TAU = 16.0
LIMIT = 7.0
SLOPE = 1.702
EPSILON = 1e-05
MESH = pl.DeviceIdType.MESH
F32 = jnp.float32
BF16 = jnp.bfloat16

N = 16
ROWS = 16
D = 4096
PIECE = 256
HALF = 2048
CAP = 4
KEYS = 256
LANES = 128
FAR = (4, 3, 5, 2, 6, 1, 7)
ALL_TP = [(d, x) for d in FAR for x in (1, 0)] + [(0, 1)]
ALL_EP = sorted(
    [(dy, dx) for dy in range(4) for dx in range(4) if dy or dx],
    key=lambda p: -sum(min(d, 4 - d) for d in p),
)


def dot(a, b):
    return jnp.dot(a, b, preferred_element_type=F32)


def dot_nt(a, b, precision=None):
    return lax.dot_general(a, b, (((1,), (1,)), ((), ())), precision=precision, preferred_element_type=F32)


def iota(shape, dim):
    return lax.broadcasted_iota(jnp.int32, shape, dim)


_scopes = []


def mark(name):
    while _scopes:
        _scopes.pop().__exit__(None, None, None)
    if name:
        _scopes.append(jax.named_scope(name))
        _scopes[-1].__enter__()


def remote(src, dst, send_sem, recv_sem, **where):
    return pltpu.make_async_remote_copy(
        src_ref=src, dst_ref=dst, send_sem=send_sem, recv_sem=recv_sem, device_id=where, device_id_type=MESH
    )


def diagonal(offset):
    return iota((ROWS, LANES), 1) == iota((ROWS, LANES), 0) + offset


def moments(part):
    mean = jnp.mean(part, axis=1, keepdims=True)
    squares = jnp.sum((part - mean) ** 2, axis=1, keepdims=True)
    line = jnp.where(diagonal(0), mean, jnp.where(diagonal(ROWS), squares, 0.0))
    return jnp.sum(line, axis=0, keepdims=True)


def merged(lines):
    lines = jnp.concatenate([lines[i] for i in range(N)], axis=0)
    total = jnp.sum(lines, axis=0, keepdims=True)
    apart = jnp.sum((lines - total / N) ** 2, axis=0, keepdims=True)

    def column(line, offset):
        return jnp.sum(jnp.where(diagonal(offset), line, 0.0), axis=1, keepdims=True)

    variance = (column(total, ROWS) + PIECE * column(apart, 0)) / D
    return column(total / N, 0), lax.rsqrt(variance + EPSILON)


def kernel(
    tok_h, qw_h, kw_h, vw_h, dd_h, du_h, db_h, st_h, ow_h, ng_h, rw_h, rt_h, glu_h, lin_h, dn_h, fg_h,
    out_ref, ns,
    tok, qw, kw, vw, dd, du, db, st, ow, ng, rw, rt, gl, dn, fg,
    sq, rq, rqk, mixed, sp, rp, rg, nrm, sd, rd, rd2, xs, sh, rh, sr, rr, sm, rm, ss, rs, lg,
    loc, out_sem, in_sem,
):
    e = lax.axis_index("ep")
    t = lax.axis_index("tp")
    z = t // 2
    c = lax.rem(t, 2)
    head = t // 4
    partner = t + 1 - 2 * c

    def tp_at(d, x):
        return 2 * lax.rem(z + d, N // 2) + lax.rem(c + x, 2)

    def ep_at(dy, dx):
        return 4 * lax.rem(e // 4 + dy, 4) + lax.rem(lax.rem(e, 4) + dx, 4)

    mark("fetch")
    head_cols = pl.ds(pl.multiple_of(head * KEYS, KEYS), KEYS)
    fetches = [
        (tok_h, tok), (qw_h, qw), (kw_h, kw), (dd_h, dd), (du_h.at[:, head_cols], du), (db_h.at[:, head_cols], db),
        (vw_h, vw), (st_h, st), (ow_h, ow), (ng_h, ng), (rw_h, rw), (rt_h, rt),
        (glu_h.at[0], gl.at[:, pl.ds(0, LANES)]), (lin_h.at[0], gl.at[:, pl.ds(LANES, LANES)]),
        (dn_h.at[0], dn), (fg_h.at[:, pl.ds(pl.multiple_of(t * PIECE, PIECE), PIECE)], fg),
    ]
    copies = [pltpu.make_async_copy(a, b, loc.at[i]) for i, (a, b) in enumerate(fetches)]
    for copy in copies:
        copy.start()

    def fetched(*which):
        for i in which:
            copies[i].wait()

    mark("barrier_signal")
    barrier = pltpu.get_barrier_semaphore()
    for p in ALL_TP:
        pl.semaphore_signal(barrier, inc=1, device_id={"tp": tp_at(*p)}, device_id_type=MESH)
    for p in ALL_EP:
        pl.semaphore_signal(barrier, inc=1, device_id={"ep": ep_at(*p)}, device_id_type=MESH)

    mark("qk_fetch_wait")
    fetched(0, 1, 2)
    mark("qk_dot")
    share = tok[:, pl.ds(pl.multiple_of(t * PIECE, PIECE), PIECE)]
    q_part = dot(share, qw[...]).astype(BF16)
    k_part = dot(share, kw[...]).astype(BF16)
    for i in range(4):
        cols = slice(i * KEYS, (i + 1) * KEYS)
        sq[0, i] = q_part[:, cols]
        sq[1, i] = k_part[:, cols]
    mark("barrier_wait")
    pl.semaphore_wait(barrier, 2 * (N - 1))
    mark("s1_send")
    pending = []

    def send(phase, src, dst, **where):
        remote(src, dst, out_sem.at[phase], in_sem.at[phase], **where).start()

    def sent(phase, like, count):
        pending.append((phase, like, count))

    def whole(phase, like, count):
        ref = like if count is None else like.at[pl.ds(0, count)]
        return remote(ref, ref, out_sem.at[phase], in_sem.at[phase], tp=partner)

    def arrived(phase, like, count):
        whole(phase, like, count).wait_recv()

    for d, x in ALL_TP:
        to = tp_at(d, x)
        send(0, sq.at[lax.rem(to, 2), to // 4], rq.at[t], tp=to)
    sent(0, rq, N - 1)
    rq[t] = sq[c, head]

    mark("decay")
    fetched(3, 4, 5, 6)
    tokens = tok[...]
    values = dot(tokens, vw[...]).astype(BF16)
    low_rank = dot_nt(tokens, dd[...])
    pre = jnp.dot(low_rank, du[...], precision=lax.Precision.HIGHEST, preferred_element_type=F32) + db[...]
    log_sig = -(jnp.maximum(-pre, 0.0) + jnp.log1p(jnp.exp(-jnp.abs(pre))))
    decay = jnp.exp(log_sig / TAU)
    hi = decay.astype(BF16)
    rest = decay - hi.astype(F32)
    mid = rest.astype(BF16)
    low = (rest - mid.astype(F32)).astype(BF16)
    thirds = jnp.concatenate([hi.astype(F32), mid.astype(F32), low.astype(F32)], axis=0)
    wide = ROWS * LANES
    ones3 = (lax.rem(iota((3 * ROWS, wide), 0), ROWS) == iota((3 * ROWS, wide), 1) // LANES).astype(BF16)
    decay_wide = dot(jnp.transpose(thirds).astype(BF16), ones3)
    mark("state_decay")
    fetched(7)
    for s in range(ROWS):
        ns[s] = decay_wide[:, s * LANES : (s + 1) * LANES] * st[s]
    own_block = iota((ROWS, wide), 0) == iota((ROWS, wide), 1) // LANES
    ones1 = own_block.astype(BF16)
    values_f = values.astype(F32)
    values_wide = jnp.where(own_block, jnp.concatenate([values_f] * ROWS, axis=1), 0.0).astype(BF16)

    mark("r1_wait")
    arrived(0, rq, N - 1)
    mark("r1_sum_r1b")
    rqk[c] = jnp.sum(rq[...].astype(F32), axis=0).astype(BF16)
    send(1, rqk.at[c], rqk.at[c], tp=partner)
    sent(1, rqk, 1)
    arrived(1, rqk, 1)
    mark("state")
    query, keys = rqk[0].astype(F32), rqk[1].astype(F32)
    update = dot(jnp.transpose(keys).astype(BF16), values_wide)
    query_wide = dot(jnp.transpose(query).astype(BF16), ones1)
    for s in range(ROWS):
        cols = slice(s * LANES, (s + 1) * LANES)
        new = ns[s] + update[:, cols]
        ns[s] = new
        mixed[s : s + 1, :] = jnp.sum(query_wide[:, cols] * new, axis=0, keepdims=True)

    mark("out_dot_s2")
    fetched(8)
    attn_part = dot((mixed[...] * KEYS ** (-0.5)).astype(BF16), ow[...]).astype(BF16)
    for i in range(N):
        sp[i] = attn_part[:, i * PIECE : (i + 1) * PIECE]
    for p in ALL_TP:
        to = tp_at(*p)
        send(2, sp.at[to], rp.at[t], tp=to)
    sent(2, sp, N - 1)
    rp[t] = sp[t]

    mark("slots")
    fetched(9, 10, 11)
    slots = N * CAP
    routed = rt[...]
    ids = iota((N, ROWS), 0)
    chosen = ((routed[0:1, :] == ids) | (routed[1:2, :] == ids)).astype(F32)
    upper = (iota((ROWS, ROWS), 0) < iota((ROWS, ROWS), 1)).astype(BF16)
    rank = dot(chosen.astype(BF16), upper)
    expand = (iota((slots, N), 0) // CAP == iota((slots, N), 1)).astype(BF16)
    here = dot(expand, chosen.astype(BF16)) > 0.5
    place = dot(expand, rank.astype(BF16))
    spread = (here & (place == lax.rem(iota((slots, ROWS), 0), CAP).astype(F32))).astype(F32)

    mark("r2_wait")
    arrived(2, rp, N - 1)
    mark("s3_send")
    rg[z] = jnp.sum(rp[...].astype(F32), axis=0).astype(BF16)
    own_cols = pl.ds(pl.multiple_of(t * PIECE, PIECE), PIECE)
    ss[0] = moments(ALPHA * tok[:, own_cols].astype(F32) + rg[z].astype(F32))
    for d in FAR:
        send(3, rg.at[z], rg.at[z], tp=tp_at(d, 0))
    for p in ALL_TP:
        send(11, ss.at[0], rs.at[0, t], tp=tp_at(*p))
    rs[0, t] = ss[0]
    sent(3, rg, N // 2 - 1)
    sent(11, rs.at[0], N - 1)
    mark("r3_wait")
    arrived(11, rs.at[0], N - 1)
    mean, scale = merged(rs[0])
    arrived(3, rg, N // 2 - 1)

    mark("norm1")
    def block(j, core):
        return pl.ds(pl.multiple_of((2 * j + core) * PIECE, PIECE), PIECE)

    for j in range(N // 2):
        hidden = ALPHA * tok[:, block(j, c)].astype(F32) + rg[j].astype(F32)
        nrm[:, j * PIECE : (j + 1) * PIECE] = ((hidden - mean) * scale * ng[:, block(j, c)]).astype(BF16)

    mark("s4_send")
    packed = dot(spread.astype(BF16), nrm[...])
    for i in range(N):
        sd[i] = packed[i * CAP : (i + 1) * CAP].astype(BF16)
    for p in ALL_EP:
        to = ep_at(*p)
        send(4, sd.at[to], rd.at[e], ep=to)
    sent(4, sd, N - 1)
    send(5, sd.at[e], rd2.at[e], tp=partner)
    sent(5, sd, 1)
    rd[e] = sd[e]

    mark("gates")
    rw_half = jnp.concatenate([rw[:, block(j, c)] for j in range(N // 2)], axis=1)
    logit_part = dot_nt(rw_half, nrm[...])
    lg[c] = jnp.concatenate([logit_part, jnp.zeros((N, LANES - ROWS), F32)], axis=1)
    send(12, lg.at[c], lg.at[c], tp=partner)
    sent(12, lg, 1)

    mark("r4_wait_fwd")
    arrived(4, rd, N - 1)
    for p in ALL_EP:
        src = ep_at(*p)
        send(6, rd.at[src], rd2.at[src], tp=partner)
    sent(6, rd, N - 1)
    mark("up_own")
    fetched(12, 13)
    for i in range(N):
        xs[i * CAP : (i + 1) * CAP, :] = rd[i].astype(F32)
    rows = xs[...].astype(BF16)
    pre_act = sum(dot(rows[:, j * PIECE : (j + 1) * PIECE], gl[block(j, c), :]) for j in range(N // 2))
    mark("r4d_wait")
    arrived(5, rd2, 1)
    arrived(6, rd2, N - 1)
    mark("up_other")
    for i in range(N):
        xs[i * CAP : (i + 1) * CAP, :] = rd2[i].astype(F32)
    rows = xs[...].astype(BF16)
    pre_act += sum(dot(rows[:, j * PIECE : (j + 1) * PIECE], gl[block(j, 1 - c), :]) for j in range(N // 2))
    glu = jnp.minimum(pre_act[:, :LANES], LIMIT)
    linear = jnp.clip(pre_act[:, LANES:], -LIMIT, LIMIT)
    act = (glu * jax.nn.sigmoid(SLOPE * glu) * (linear + 1.0)).astype(BF16)

    mark("down")
    fetched(14)
    theirs = [dot(act, dn[:, block(j, 1 - c)]) for j in range(N // 2)]
    for j in range(N // 2):
        sh[j] = theirs[j].astype(BF16)
    send(7, sh, rh, tp=partner)
    sent(7, sh, None)
    mine = [dot(act, dn[:, block(j, c)]) for j in range(N // 2)]
    mark("down_wait")
    arrived(7, rh, None)
    mark("down_sum")
    for j in range(N // 2):
        total = (mine[j] + rh[j].astype(F32)).astype(BF16)
        for i in range(N):
            sr[i, :, j * PIECE : (j + 1) * PIECE] = total[i * CAP : (i + 1) * CAP]
    mark("s6_send")
    for p in ALL_EP:
        to = ep_at(*p)
        send(8, sr.at[to], rr.at[e], ep=to)
    sent(8, sr, N - 1)
    rr[e] = sr[e]
    mark("gates2")
    arrived(12, lg, 1)
    logits = (lg[0] + lg[1])[:, :ROWS]
    raised = jnp.where(chosen > 0.5, jnp.exp(logits), 0.0)
    gates = raised / jnp.sum(raised, axis=0, keepdims=True)
    gate_rows = spread * jnp.dot(
        expand.astype(F32), gates, precision=lax.Precision.HIGHEST, preferred_element_type=F32
    )
    gate_cols = jnp.transpose(gate_rows)
    gate_hi = gate_cols.astype(BF16)
    gate_lo = (gate_cols - gate_hi.astype(F32)).astype(BF16)

    mark("r6_wait")
    arrived(8, rr, N - 1)

    mark("mix_s7")
    for i in range(N):
        xs[i * CAP : (i + 1) * CAP, :] = rr[i].astype(F32)
    back = xs[...].astype(BF16)
    mix = (dot(gate_hi, back) + dot(gate_lo, back)).astype(BF16)
    for j in range(N // 2):
        sm[j] = mix[:, j * PIECE : (j + 1) * PIECE]
    for d in FAR:
        to = lax.rem(z + d, N // 2)
        send(9, sm.at[to], rm.at[z], tp=2 * to + c)
    sent(9, sm, N // 2 - 1)
    rm[z] = sm[z]
    mark("r7_wait")
    arrived(9, rm, N // 2 - 1)
    mark("stats_s8")
    own = nrm[:, pl.ds(pl.multiple_of(z * PIECE, PIECE), PIECE)].astype(F32)
    u = ALPHA * own + jnp.sum(rm[...].astype(F32), axis=0)

    ss[1] = moments(u)
    for p in ALL_TP:
        send(10, ss.at[1], rs.at[1, t], tp=tp_at(*p))
    sent(10, rs.at[1], N - 1)
    rs[1, t] = ss[1]
    mark("r8_wait")
    fetched(15)
    arrived(10, rs.at[1], N - 1)
    mark("final")
    mean, scale = merged(rs[1])
    out_ref[...] = ((u - mean) * scale * fg[...]).astype(BF16)

    mark("drain")
    for phase, like, count in pending:
        whole(phase, like, count).wait_send()
    mark(None)


def written_out(out, state, out_h, state_h, sems):
    copies = [
        pltpu.make_async_copy(state, state_h, sems.at[0]),
        pltpu.make_async_copy(out, out_h, sems.at[1]),
    ]
    for copy in copies:
        copy.start()
    for copy in copies:
        copy.wait()


def step(
    tokens, query_weight, key_weight, value_weight, decay_down, decay_up, decay_bias, old_state, out_weight,
    norm_gain, router_weight, routing, glu_weight, linear_weight, down_weight, final_gain,
):
    hbm = pl.BlockSpec(memory_space=pl.ANY)
    vmem, dma = pltpu.VMEM, pltpu.SemaphoreType.DMA
    results = pl.pallas_call(
        kernel,
        out_shape=(
            pltpu.VMEM((ROWS, PIECE), BF16),
            pltpu.VMEM(old_state.shape, F32),
        ),
        in_specs=[hbm] * 16,
        out_specs=(pl.BlockSpec(memory_space=pltpu.VMEM), pl.BlockSpec(memory_space=pltpu.VMEM)),
        scratch_shapes=[
            vmem((ROWS, D), BF16), vmem((PIECE, 1024), BF16), vmem((PIECE, 1024), BF16), vmem((D, LANES), BF16),
            vmem((N, D), BF16), vmem((16, KEYS), F32), vmem((1, KEYS), F32), vmem((ROWS, KEYS, LANES), F32),
            vmem((LANES, D), BF16), vmem((1, D), F32), vmem((N, D), BF16), vmem((2, ROWS), jnp.int32),
            vmem((D, 2 * LANES), BF16), vmem((LANES, D), BF16), vmem((1, PIECE), F32),
            vmem((2, 4, ROWS, KEYS), BF16), vmem((N, ROWS, KEYS), BF16), vmem((2, ROWS, KEYS), BF16),
            vmem((ROWS, LANES), F32), vmem((N, ROWS, PIECE), BF16), vmem((N, ROWS, PIECE), BF16),
            vmem((N // 2, ROWS, PIECE), BF16), vmem((ROWS, HALF), BF16),
            vmem((N, CAP, HALF), BF16), vmem((N, CAP, HALF), BF16), vmem((N, CAP, HALF), BF16),
            vmem((N * CAP, HALF), F32), vmem((N // 2, N * CAP, PIECE), BF16), vmem((N // 2, N * CAP, PIECE), BF16),
            vmem((N, CAP, HALF), BF16), vmem((N, CAP, HALF), BF16), vmem((N // 2, ROWS, PIECE), BF16),
            vmem((N // 2, ROWS, PIECE), BF16), vmem((2, 1, LANES), F32), vmem((2, N, 1, LANES), F32), vmem((2, N, LANES), F32),
            dma((16,)), dma((13,)), dma((13,)),
        ],
        compiler_params=pltpu.CompilerParams(
            collective_id=0, has_side_effects=True, vmem_limit_bytes=60 * 1024 * 1024
        ),
        name="decode_step",
    )(
        tokens, query_weight, key_weight, value_weight, decay_down.T, decay_up, decay_bias.reshape(1, -1), old_state,
        out_weight, norm_gain.reshape(1, -1), router_weight.T, routing.T, glu_weight, linear_weight, down_weight,
        final_gain.reshape(1, -1),
    )
    results = [pltpu.with_memory_space_constraint(r, pltpu.VMEM) for r in results]
    return pl.pallas_call(
        written_out,
        out_shape=tuple(jax.ShapeDtypeStruct(r.shape, r.dtype) for r in results),
        in_specs=[pl.BlockSpec(memory_space=pltpu.VMEM)] * 2,
        out_specs=(hbm, hbm),
        scratch_shapes=[dma((2,))],
        name="written_out",
    )(*results)


def solution(mesh):
    in_specs = (
        P("ep", None), P("tp", None), P("tp", None), P(None, "tp"), P(), P(), P(), P("ep", None, "tp"), P("tp", None),
        P(), P(), P("ep", None), P("ep", None, "tp"), P("ep", None, "tp"), P("ep", "tp", None), P(),
    )
    out_specs = (P("ep", "tp"), P("ep", None, "tp"))
    return jax.shard_map(step, mesh=mesh, in_specs=in_specs, out_specs=out_specs, check_vma=False)
```

```python
import functools

import jax
import jax.numpy as jnp
from jax import lax
from jax.experimental import pallas as pl
from jax.experimental.pallas import tpu as pltpu
from jax.sharding import PartitionSpec as P

ALPHA = 2.0**0.25
TAU = 16.0
LIMIT = 7.0
SLOPE = 1.702
EPSILON = 1e-05
MESH = pl.DeviceIdType.MESH
F32 = jnp.float32
BF16 = jnp.bfloat16

N = 16
ROWS = 16
D = 4096
PIECE = 256
HALF = 2048
CAP = 4
KEYS = 256
LANES = 128
FAR = (4, 3, 5, 2, 6, 1, 7)
ALL_TP = [(d, x) for d in FAR for x in (1, 0)] + [(0, 1)]
ALL_EP = sorted(
    [(dy, dx) for dy in range(4) for dx in range(4) if dy or dx],
    key=lambda p: -sum(min(d, 4 - d) for d in p),
)


def dot(a, b):
    return jnp.dot(a, b, preferred_element_type=F32)


def dot_nt(a, b, precision=None):
    return lax.dot_general(a, b, (((1,), (1,)), ((), ())), precision=precision, preferred_element_type=F32)


def iota(shape, dim):
    return lax.broadcasted_iota(jnp.int32, shape, dim)


_scopes = []


def mark(name):
    while _scopes:
        _scopes.pop().__exit__(None, None, None)
    if name:
        _scopes.append(jax.named_scope(name))
        _scopes[-1].__enter__()


def remote(src, dst, send_sem, recv_sem, **where):
    return pltpu.make_async_remote_copy(
        src_ref=src, dst_ref=dst, send_sem=send_sem, recv_sem=recv_sem, device_id=where, device_id_type=MESH
    )


def diagonal(offset):
    return iota((ROWS, LANES), 1) == iota((ROWS, LANES), 0) + offset


def moments(part):
    mean = jnp.mean(part, axis=1, keepdims=True)
    squares = jnp.sum((part - mean) ** 2, axis=1, keepdims=True)
    line = jnp.where(diagonal(0), mean, jnp.where(diagonal(ROWS), squares, 0.0))
    return jnp.sum(line, axis=0, keepdims=True)


def merged(lines):
    lines = jnp.concatenate([lines[i] for i in range(N)], axis=0)
    total = jnp.sum(lines, axis=0, keepdims=True)
    apart = jnp.sum((lines - total / N) ** 2, axis=0, keepdims=True)

    def column(line, offset):
        return jnp.sum(jnp.where(diagonal(offset), line, 0.0), axis=1, keepdims=True)

    variance = (column(total, ROWS) + PIECE * column(apart, 0)) / D
    return column(total / N, 0), lax.rsqrt(variance + EPSILON)


def kernel(
    tok_h, qw_h, kw_h, vw_h, dd_h, du_h, db_h, st_h, ow_h, ng_h, rw_h, rt_h, glu_h, lin_h, dn_h, fg_h,
    out_ref, ns,
    tok, qw, kw, vw, dd, du, db, st, ow, ng, rw, rt, gl, dn, fg, decayed,
    sq, rq, rqk, mixed, sp, rp, rg, nrm, sd, rd, su, ru, sr, rr, sm, rm, ss, rs, lg,
    loc, out_sem, in_sem,
):
    e = lax.axis_index("ep")
    t = lax.axis_index("tp")
    z = t // 2
    c = lax.rem(t, 2)
    head = t // 4
    partner = t + 1 - 2 * c

    def tp_at(d, x):
        return 2 * lax.rem(z + d, N // 2) + lax.rem(c + x, 2)

    def ep_at(dy, dx):
        return 4 * lax.rem(e // 4 + dy, 4) + lax.rem(lax.rem(e, 4) + dx, 4)

    mark("fetch")
    head_cols = pl.ds(pl.multiple_of(head * KEYS, KEYS), KEYS)
    fetches = [
        (tok_h, tok), (qw_h, qw), (kw_h, kw), (dd_h, dd), (du_h.at[:, head_cols], du), (db_h.at[:, head_cols], db),
        (vw_h, vw), (st_h, st), (ow_h, ow), (ng_h, ng), (rw_h, rw), (rt_h, rt),
        (fg_h.at[:, pl.ds(pl.multiple_of(t * PIECE, PIECE), PIECE)], fg),
    ]
    copies = [pltpu.make_async_copy(a, b, loc.at[i]) for i, (a, b) in enumerate(fetches)]
    for copy in copies:
        copy.start()

    units = pl.ds(pl.multiple_of(c * LANES, LANES), LANES)
    linear_units = pl.ds(pl.multiple_of((2 + c) * LANES, LANES), LANES)

    def expert_weights(core):
        blocks = [(glu_h.at[:, core], gl.at[:, :, units]), (lin_h.at[:, core], gl.at[:, :, linear_units])]
        for j in range(N // 2):
            cols = pl.ds(pl.multiple_of((2 * j + core) * PIECE, PIECE), PIECE)
            blocks.append((dn_h.at[0, :, cols], dn.at[j, units, :]))
        return blocks

    own_weights = [pltpu.make_async_copy(a, b, loc.at[13 + i]) for i, (a, b) in enumerate(expert_weights(c))]

    def fetched(*which):
        for i in which:
            copies[i].wait()

    mark("barrier_signal")
    barrier = pltpu.get_barrier_semaphore()
    for p in ALL_TP:
        pl.semaphore_signal(barrier, inc=1, device_id={"tp": tp_at(*p)}, device_id_type=MESH)
    for p in ALL_EP:
        pl.semaphore_signal(barrier, inc=1, device_id={"ep": ep_at(*p)}, device_id_type=MESH)

    mark("qk_fetch_wait")
    fetched(0, 1, 2)
    mark("qk_dot")
    share = tok[:, pl.ds(pl.multiple_of(t * PIECE, PIECE), PIECE)]
    q_part = dot(share, qw[...]).astype(BF16)
    k_part = dot(share, kw[...]).astype(BF16)
    for i in range(4):
        cols = slice(i * KEYS, (i + 1) * KEYS)
        sq[0, i] = q_part[:, cols]
        sq[1, i] = k_part[:, cols]
    mark("barrier_wait")
    pl.semaphore_wait(barrier, 2 * (N - 1))
    mark("s1_send")
    pending = []

    def send(phase, src, dst, **where):
        remote(src, dst, out_sem.at[phase], in_sem.at[phase], **where).start()

    def sent(phase, like, count):
        pending.append((phase, like, count))

    def whole(phase, like, count):
        ref = like if count is None else like.at[pl.ds(0, count)]
        return remote(ref, ref, out_sem.at[phase], in_sem.at[phase], tp=partner)

    def arrived(phase, like, count):
        whole(phase, like, count).wait_recv()

    for d, x in ALL_TP:
        to = tp_at(d, x)
        send(0, sq.at[lax.rem(to, 2), to // 4], rq.at[t], tp=to)
    sent(0, rq, N - 1)
    for copy in own_weights:
        copy.start()
    for i, (mine, theirs) in enumerate(expert_weights(1 - c)):
        send(min(13 + i, 15), mine, theirs, tp=partner)
    rq[t] = sq[c, head]

    mark("decay")
    fetched(3, 4, 5, 6)
    tokens = tok[...]
    values = dot(tokens, vw[...]).astype(BF16)
    low_rank = dot_nt(tokens, dd[...])
    pre = jnp.dot(low_rank, du[...], precision=lax.Precision.HIGHEST, preferred_element_type=F32) + db[...]
    log_sig = -(jnp.maximum(-pre, 0.0) + jnp.log1p(jnp.exp(-jnp.abs(pre))))
    decay = jnp.exp(log_sig / TAU)
    hi = decay.astype(BF16)
    rest = decay - hi.astype(F32)
    mid = rest.astype(BF16)
    low = (rest - mid.astype(F32)).astype(BF16)
    thirds = jnp.concatenate([hi.astype(F32), mid.astype(F32), low.astype(F32)], axis=0)
    wide = ROWS * LANES
    ones3 = (lax.rem(iota((3 * ROWS, wide), 0), ROWS) == iota((3 * ROWS, wide), 1) // LANES).astype(BF16)
    decay_wide = dot(jnp.transpose(thirds).astype(BF16), ones3)
    mark("state_decay")
    fetched(7)
    for s in range(ROWS):
        decayed[s] = decay_wide[:, s * LANES : (s + 1) * LANES] * st[s]
    own_block = iota((ROWS, wide), 0) == iota((ROWS, wide), 1) // LANES
    ones1 = own_block.astype(BF16)
    values_f = values.astype(F32)
    values_wide = jnp.where(own_block, jnp.concatenate([values_f] * ROWS, axis=1), 0.0).astype(BF16)

    mark("r1_wait")
    arrived(0, rq, N - 1)
    mark("r1_sum_r1b")
    rqk[c] = jnp.sum(rq[...].astype(F32), axis=0).astype(BF16)
    send(1, rqk.at[c], rqk.at[c], tp=partner)
    sent(1, rqk, 1)
    arrived(1, rqk, 1)
    mark("state")
    query, keys = rqk[0].astype(F32), rqk[1].astype(F32)
    query_wide = dot(jnp.transpose(query).astype(BF16), ones1)
    for s in range(ROWS):
        cols = slice(s * LANES, (s + 1) * LANES)
        mixed[s : s + 1, :] = jnp.sum(query_wide[:, cols] * decayed[s], axis=0, keepdims=True)
    match = jnp.sum(query * keys, axis=1, keepdims=True)
    mark("out_dot_s2")
    fetched(8)
    readout = (mixed[...] + match * values_f) * KEYS ** (-0.5)
    attn_part = dot(readout.astype(BF16), ow[...]).astype(BF16)
    for i in range(N):
        sp[i] = attn_part[:, i * PIECE : (i + 1) * PIECE]
    for p in ALL_TP:
        to = tp_at(*p)
        send(2, sp.at[to], rp.at[t], tp=to)
    sent(2, sp, N - 1)
    rp[t] = sp[t]

    mark("update")
    update = dot(jnp.transpose(keys).astype(BF16), values_wide)
    for s in range(ROWS):
        ns[s] = decayed[s] + update[:, s * LANES : (s + 1) * LANES]
    mark("slots")
    fetched(9, 10, 11)
    slots = N * CAP
    routed = rt[...]
    ids = iota((N, ROWS), 0)
    chosen = ((routed[0:1, :] == ids) | (routed[1:2, :] == ids)).astype(F32)
    upper = (iota((ROWS, ROWS), 0) < iota((ROWS, ROWS), 1)).astype(BF16)
    rank = dot(chosen.astype(BF16), upper)
    expand = (iota((slots, N), 0) // CAP == iota((slots, N), 1)).astype(BF16)
    here = dot(expand, chosen.astype(BF16)) > 0.5
    place = dot(expand, rank.astype(BF16))
    spread = (here & (place == lax.rem(iota((slots, ROWS), 0), CAP).astype(F32))).astype(F32)

    mark("r2_wait")
    arrived(2, rp, N - 1)
    mark("s3_send")
    rg[z] = jnp.sum(rp[...].astype(F32), axis=0).astype(BF16)
    own_cols = pl.ds(pl.multiple_of(t * PIECE, PIECE), PIECE)
    ss[0] = moments(ALPHA * tok[:, own_cols].astype(F32) + rg[z].astype(F32))
    for d in FAR:
        send(3, rg.at[z], rg.at[z], tp=tp_at(d, 0))
    for p in ALL_TP:
        send(11, ss.at[0], rs.at[0, t], tp=tp_at(*p))
    rs[0, t] = ss[0]
    sent(3, rg, N // 2 - 1)
    sent(11, rs.at[0], N - 1)
    mark("r3_wait")
    arrived(11, rs.at[0], N - 1)
    mean, scale = merged(rs[0])
    arrived(3, rg, N // 2 - 1)

    mark("norm1")
    def block(j, core):
        return pl.ds(pl.multiple_of((2 * j + core) * PIECE, PIECE), PIECE)

    for j in range(N // 2):
        hidden = ALPHA * tok[:, block(j, c)].astype(F32) + rg[j].astype(F32)
        nrm[:, j * PIECE : (j + 1) * PIECE] = ((hidden - mean) * scale * ng[:, block(j, c)]).astype(BF16)

    mark("s4_send")
    sd[...] = dot(spread.astype(BF16), nrm[...]).astype(BF16).reshape(N, CAP, HALF)
    for p in ALL_EP:
        to = ep_at(*p)
        send(4, sd.at[to], rd.at[e], ep=to)
    sent(4, sd, N - 1)
    rd[e] = sd[e]

    mark("gates")
    rw_half = jnp.concatenate([rw[:, block(j, c)] for j in range(N // 2)], axis=1)
    logit_part = dot_nt(rw_half, nrm[...])
    lg[c] = jnp.concatenate([logit_part, jnp.zeros((N, LANES - ROWS), F32)], axis=1)
    send(12, lg.at[c], lg.at[c], tp=partner)
    sent(12, lg, 1)

    mark("r4_wait_fwd")
    arrived(4, rd, N - 1)
    mark("up")
    rows = rd[...].reshape(N * CAP, HALF)
    for copy in own_weights[:2]:
        copy.wait()
    arrived(13, gl.at[:, :, pl.ds(0, LANES)], None)
    arrived(14, gl.at[:, :, pl.ds(0, LANES)], None)
    su[...] = dot(rows, gl[...].reshape(HALF, 4 * LANES))
    send(5, su, ru, tp=partner)
    sent(5, su, None)
    mark("up_wait")
    arrived(5, ru, None)
    mark("down")
    pre_act = su[...] + ru[...]
    glu = jnp.minimum(pre_act[:, : 2 * LANES], LIMIT)
    linear = jnp.clip(pre_act[:, 2 * LANES :], -LIMIT, LIMIT)
    act = (glu * jax.nn.sigmoid(SLOPE * glu) * (linear + 1.0)).astype(BF16)

    mark("down")
    for copy in own_weights[2:]:
        copy.wait()
    arrived(15, dn.at[:, pl.ds(0, LANES), :], None)
    for j in range(N // 2):
        sr[:, :, j * PIECE : (j + 1) * PIECE] = dot(act, dn[j]).astype(BF16).reshape(N, CAP, PIECE)
    mark("s6_send")
    for p in ALL_EP:
        to = ep_at(*p)
        send(8, sr.at[to], rr.at[e], ep=to)
    sent(8, sr, N - 1)
    rr[e] = sr[e]
    mark("gates2")
    arrived(12, lg, 1)
    logits = (lg[0] + lg[1])[:, :ROWS]
    raised = jnp.where(chosen > 0.5, jnp.exp(logits), 0.0)
    gates = raised / jnp.sum(raised, axis=0, keepdims=True)
    gate_rows = spread * jnp.dot(
        expand.astype(F32), gates, precision=lax.Precision.HIGHEST, preferred_element_type=F32
    )
    gate_cols = jnp.transpose(gate_rows)
    gate_hi = gate_cols.astype(BF16)
    gate_lo = (gate_cols - gate_hi.astype(F32)).astype(BF16)

    mark("r6_wait")
    arrived(8, rr, N - 1)

    mark("mix_s7")
    back = rr[...].reshape(N * CAP, HALF)
    mix = (dot(gate_hi, back) + dot(gate_lo, back)).astype(BF16)
    for j in range(N // 2):
        sm[j] = mix[:, j * PIECE : (j + 1) * PIECE]
    for d in FAR:
        to = lax.rem(z + d, N // 2)
        send(9, sm.at[to], rm.at[z], tp=2 * to + c)
    sent(9, sm, N // 2 - 1)
    rm[z] = sm[z]
    mark("r7_wait")
    arrived(9, rm, N // 2 - 1)
    mark("stats_s8")
    own = nrm[:, pl.ds(pl.multiple_of(z * PIECE, PIECE), PIECE)].astype(F32)
    u = ALPHA * own + jnp.sum(rm[...].astype(F32), axis=0)

    ss[1] = moments(u)
    for p in ALL_TP:
        send(10, ss.at[1], rs.at[1, t], tp=tp_at(*p))
    sent(10, rs.at[1], N - 1)
    rs[1, t] = ss[1]
    mark("r8_wait")
    fetched(12)
    arrived(10, rs.at[1], N - 1)
    mark("final")
    mean, scale = merged(rs[1])
    out_ref[...] = ((u - mean) * scale * fg[...]).astype(BF16)

    mark("drain")
    sent(13, gl.at[:, :, pl.ds(0, LANES)], None)
    sent(14, gl.at[:, :, pl.ds(0, LANES)], None)
    sent(15, dn.at[:, pl.ds(0, LANES), :], None)
    for phase, like, count in pending:
        whole(phase, like, count).wait_send()
    mark(None)


def written_out(out, state, out_h, state_h, sems):
    rows = [pl.ds(2 * i, 2) for i in range(ROWS // 2)]
    copies = [pltpu.make_async_copy(state.at[r], state_h.at[r], sems.at[i]) for i, r in enumerate(rows)]
    copies.append(pltpu.make_async_copy(out, out_h, sems.at[ROWS // 2]))
    for copy in copies:
        copy.start()
    for copy in copies:
        copy.wait()


def step(
    tokens, query_weight, key_weight, value_weight, decay_down, decay_up, decay_bias, old_state, out_weight,
    norm_gain, router_weight, routing, glu_weight, linear_weight, down_weight, final_gain,
):
    hbm = pl.BlockSpec(memory_space=pl.ANY)

    def in_blocks(weight):
        return weight.reshape(N // 2, 2, PIECE, LANES)

    vmem, dma = pltpu.VMEM, pltpu.SemaphoreType.DMA
    results = pl.pallas_call(
        kernel,
        out_shape=(
            pltpu.VMEM((ROWS, PIECE), BF16),
            pltpu.VMEM(old_state.shape, F32),
        ),
        in_specs=[hbm] * 16,
        out_specs=(pl.BlockSpec(memory_space=pltpu.VMEM), pl.BlockSpec(memory_space=pltpu.VMEM)),
        scratch_shapes=[
            vmem((ROWS, D), BF16), vmem((PIECE, 1024), BF16), vmem((PIECE, 1024), BF16), vmem((D, LANES), BF16),
            vmem((N, D), BF16), vmem((16, KEYS), F32), vmem((1, KEYS), F32), vmem((ROWS, KEYS, LANES), F32),
            vmem((LANES, D), BF16), vmem((1, D), F32), vmem((N, D), BF16), vmem((2, ROWS), jnp.int32),
            vmem((N // 2, PIECE, 4 * LANES), BF16), vmem((N // 2, 2 * LANES, PIECE), BF16), vmem((1, PIECE), F32), vmem((ROWS, KEYS, LANES), F32),
            vmem((2, 4, ROWS, KEYS), BF16), vmem((N, ROWS, KEYS), BF16), vmem((2, ROWS, KEYS), BF16),
            vmem((ROWS, LANES), F32), vmem((N, ROWS, PIECE), BF16), vmem((N, ROWS, PIECE), BF16),
            vmem((N // 2, ROWS, PIECE), BF16), vmem((ROWS, HALF), BF16),
            vmem((N, CAP, HALF), BF16), vmem((N, CAP, HALF), BF16),
            vmem((N * CAP, 4 * LANES), F32), vmem((N * CAP, 4 * LANES), F32),
            vmem((N, CAP, HALF), BF16), vmem((N, CAP, HALF), BF16), vmem((N // 2, ROWS, PIECE), BF16),
            vmem((N // 2, ROWS, PIECE), BF16), vmem((2, 1, LANES), F32), vmem((2, N, 1, LANES), F32), vmem((2, N, LANES), F32),
            dma((24,)), dma((16,)), dma((16,)),
        ],
        compiler_params=pltpu.CompilerParams(
            collective_id=0, has_side_effects=True, vmem_limit_bytes=60 * 1024 * 1024
        ),
        name="decode_step",
    )(
        tokens, query_weight, key_weight, value_weight, decay_down.T, decay_up, decay_bias.reshape(1, -1), old_state,
        out_weight, norm_gain.reshape(1, -1), router_weight.T, routing.T, in_blocks(glu_weight), in_blocks(linear_weight), down_weight,
        final_gain.reshape(1, -1),
    )
    results = [pltpu.with_memory_space_constraint(r, pltpu.VMEM) for r in results]
    return pl.pallas_call(
        written_out,
        out_shape=tuple(jax.ShapeDtypeStruct(r.shape, r.dtype) for r in results),
        in_specs=[pl.BlockSpec(memory_space=pltpu.VMEM)] * 2,
        out_specs=(hbm, hbm),
        scratch_shapes=[dma((ROWS // 2 + 1,))],
        name="written_out",
    )(*results)


def solution(mesh):
    in_specs = (
        P("ep", None), P("tp", None), P("tp", None), P(None, "tp"), P(), P(), P(), P("ep", None, "tp"), P("tp", None),
        P(), P(), P("ep", None), P("ep", None, "tp"), P("ep", None, "tp"), P("ep", "tp", None), P(),
    )
    out_specs = (P("ep", "tp"), P("ep", None, "tp"))
    return jax.shard_map(step, mesh=mesh, in_specs=in_specs, out_specs=out_specs, check_vma=False)
```

```python
import functools

import jax
import jax.numpy as jnp
from jax import lax
from jax.experimental import pallas as pl
from jax.experimental.pallas import tpu as pltpu
from jax.sharding import PartitionSpec as P

ALPHA = 2.0**0.25
TAU = 16.0
LIMIT = 7.0
SLOPE = 1.702
EPSILON = 1e-05
MESH = pl.DeviceIdType.MESH
F32 = jnp.float32
BF16 = jnp.bfloat16

N = 16
ROWS = 16
D = 4096
PIECE = 256
HALF = 2048
CAP = 4
PART = 8
KEYS = 256
LANES = 128
FAR = (4, 3, 5, 2, 6, 1, 7)
ALL_TP = [(d, x) for d in FAR for x in (1, 0)] + [(0, 1)]
ALL_EP = sorted(
    [(dy, dx) for dy in range(4) for dx in range(4) if dy or dx],
    key=lambda p: -sum(min(d, 4 - d) for d in p),
)


def dot(a, b):
    return jnp.dot(a, b, preferred_element_type=F32)


def dot_nt(a, b, precision=None):
    return lax.dot_general(a, b, (((1,), (1,)), ((), ())), precision=precision, preferred_element_type=F32)


def iota(shape, dim):
    return lax.broadcasted_iota(jnp.int32, shape, dim)


_scopes = []


def mark(name):
    while _scopes:
        _scopes.pop().__exit__(None, None, None)
    if name:
        _scopes.append(jax.named_scope(name))
        _scopes[-1].__enter__()


def remote(src, dst, send_sem, recv_sem, **where):
    return pltpu.make_async_remote_copy(
        src_ref=src, dst_ref=dst, send_sem=send_sem, recv_sem=recv_sem, device_id=where, device_id_type=MESH
    )


def diagonal(offset):
    return iota((ROWS, LANES), 1) == iota((ROWS, LANES), 0) + offset


def moments(part):
    mean = jnp.mean(part, axis=1, keepdims=True)
    squares = jnp.sum((part - mean) ** 2, axis=1, keepdims=True)
    line = jnp.where(diagonal(0), mean, jnp.where(diagonal(ROWS), squares, 0.0))
    return jnp.sum(line, axis=0, keepdims=True)


def merged(lines):
    lines = jnp.concatenate([lines[i] for i in range(N)], axis=0)
    total = jnp.sum(lines, axis=0, keepdims=True)
    apart = jnp.sum((lines - total / N) ** 2, axis=0, keepdims=True)

    def column(line, offset):
        return jnp.sum(jnp.where(diagonal(offset), line, 0.0), axis=1, keepdims=True)

    variance = (column(total, ROWS) + PIECE * column(apart, 0)) / D
    return column(total / N, 0), lax.rsqrt(variance + EPSILON)


def kernel(
    tok_h, qw_h, kw_h, vw_h, dd_h, du_h, db_h, st_h, ow_h, ng_h, rw_h, rt_h, glu_h, lin_h, dn_h, fg_h,
    out_ref, ns,
    tok, qw, kw, vw, dd, du, db, st, ow, ng, rw, rt, gl, dn, fg, tok_part, decayed,
    sq, rq, vals, val_out, mixed, sp, rp, rg, hid, nrm, sd, rd, su, ru, sr, rr, sm, rm, ss, rs, ns_in,
    loc, out_sem, in_sem,
):
    e = lax.axis_index("ep")
    t = lax.axis_index("tp")
    z = t // 2
    c = lax.rem(t, 2)
    head = t // 4
    partner = t + 1 - 2 * c

    def tp_at(d, x):
        return 2 * lax.rem(z + d, N // 2) + lax.rem(c + x, 2)

    def ep_at(dy, dx):
        return 4 * lax.rem(e // 4 + dy, 4) + lax.rem(lax.rem(e, 4) + dx, 4)

    mark("fetch")
    units = pl.ds(pl.multiple_of(c * LANES, LANES), LANES)
    linear_units = pl.ds(pl.multiple_of((2 + c) * LANES, LANES), LANES)

    def rows_of(core):
        return pl.ds(pl.multiple_of(core * PART, PART), PART)

    head_cols = pl.ds(pl.multiple_of(head * KEYS, KEYS), KEYS)
    fetches = [
        (tok_h, tok), (qw_h, qw), (kw_h, kw), (dd_h, dd), (du_h.at[:, head_cols], du), (db_h.at[:, head_cols], db),
        (vw_h, vw), (st_h.at[rows_of(c)], st.at[c]), (ow_h, ow.at[units, :]), (ng_h, ng), (rw_h, rw), (rt_h, rt),
        (fg_h.at[:, pl.ds(pl.multiple_of(t * PIECE, PIECE), PIECE)], fg),
        (tok_h.at[rows_of(c), :], tok_part),
    ]
    copies = [pltpu.make_async_copy(a, b, loc.at[i]) for i, (a, b) in enumerate(fetches)]
    for copy in copies:
        copy.start()


    def expert_weights(core):
        blocks = [(glu_h.at[:, core], gl.at[:, :, units]), (lin_h.at[:, core], gl.at[:, :, linear_units])]
        for j in range(N // 2):
            cols = pl.ds(pl.multiple_of((2 * j + core) * PIECE, PIECE), PIECE)
            blocks.append((dn_h.at[0, :, cols], dn.at[j, units, :]))
        return blocks

    own_weights = [pltpu.make_async_copy(a, b, loc.at[14 + i]) for i, (a, b) in enumerate(expert_weights(c))]

    def fetched(*which):
        for i in which:
            copies[i].wait()

    mark("barrier_signal")
    barrier = pltpu.get_barrier_semaphore()
    for p in ALL_TP:
        pl.semaphore_signal(barrier, inc=1, device_id={"tp": tp_at(*p)}, device_id_type=MESH)
    for p in ALL_EP:
        pl.semaphore_signal(barrier, inc=1, device_id={"ep": ep_at(*p)}, device_id_type=MESH)

    mark("qk_fetch_wait")
    fetched(0, 1, 2)
    mark("qk_dot")
    share = tok[:, pl.ds(pl.multiple_of(t * PIECE, PIECE), PIECE)]
    q_part = dot(share, qw[...]).astype(BF16)
    k_part = dot(share, kw[...]).astype(BF16)
    for i in range(4):
        cols = slice(i * KEYS, (i + 1) * KEYS)
        both = jnp.concatenate([q_part[:, cols], k_part[:, cols]], axis=1)
        sq[0, i] = both[:PART]
        sq[1, i] = both[PART:]
    mark("barrier_wait")
    pl.semaphore_wait(barrier, 2 * (N - 1))
    mark("s1_send")
    pending = []

    def send(phase, src, dst, **where):
        remote(src, dst, out_sem.at[phase], in_sem.at[phase], **where).start()

    def sent(phase, like, count):
        pending.append((phase, like, count))

    def whole(phase, like, count):
        ref = like if count is None else like.at[pl.ds(0, count)]
        return remote(ref, ref, out_sem.at[phase], in_sem.at[phase], tp=partner)

    def arrived(phase, like, count):
        whole(phase, like, count).wait_recv()

    for d, x in ALL_TP:
        to = tp_at(d, x)
        send(0, sq.at[lax.rem(to, 2), to // 4], rq.at[t], tp=to)
    sent(0, rq, N - 1)
    send(11, st_h.at[rows_of(1 - c)], st.at[c], tp=partner)
    send(12, ow_h, ow.at[units, :], tp=partner)
    rq[t] = sq[c, head]

    mark("decay")
    fetched(3, 4, 5, 6, 13)
    values = dot(tok[...], vw[...]).astype(BF16).astype(F32)
    mine_first = c == 0
    val_out[...] = jnp.where(mine_first, values[PART:], values[:PART])
    vals[c] = jnp.where(mine_first, values[:PART], values[PART:])
    send(1, val_out, vals.at[c], tp=partner)
    sent(1, val_out, None)
    low_rank = dot_nt(tok_part[...], dd[...])
    pre = jnp.dot(low_rank, du[...], precision=lax.Precision.HIGHEST, preferred_element_type=F32) + db[...]
    log_sig = -(jnp.maximum(-pre, 0.0) + jnp.log1p(jnp.exp(-jnp.abs(pre))))
    decay = jnp.exp(log_sig / TAU)
    hi = decay.astype(BF16)
    rest = decay - hi.astype(F32)
    mid = rest.astype(BF16)
    low = (rest - mid.astype(F32)).astype(BF16)
    thirds = jnp.concatenate([hi.astype(F32), mid.astype(F32), low.astype(F32)], axis=0)
    wide = PART * LANES
    ones3 = (lax.rem(iota((3 * PART, wide), 0), PART) == iota((3 * PART, wide), 1) // LANES).astype(BF16)
    decay_wide = dot(jnp.transpose(thirds).astype(BF16), ones3)
    mark("state_decay")
    fetched(7)
    arrived(11, st.at[0], None)
    for g in range(2):
        for s in range(PART):
            decayed[g, s] = decay_wide[:, s * LANES : (s + 1) * LANES] * st[g, s]
    own_block = iota((PART, wide), 0) == iota((PART, wide), 1) // LANES
    ones1 = own_block.astype(BF16)
    arrived(1, val_out, None)
    values_f = jnp.concatenate([vals[0], vals[1]], axis=1)
    values_wide = jnp.concatenate(
        [jnp.where(own_block, jnp.concatenate([vals[g]] * PART, axis=1), 0.0).astype(BF16) for g in range(2)], axis=1
    )
    mark("r1_wait")
    arrived(0, rq, N - 1)
    mark("state")
    query_keys = jnp.sum(rq[...].astype(F32), axis=0).astype(BF16).astype(F32)
    query, keys = query_keys[:, :KEYS], query_keys[:, KEYS:]
    query_wide = dot(jnp.transpose(query).astype(BF16), ones1)
    for g in range(2):
        for s in range(PART):
            spread_query = query_wide[:, s * LANES : (s + 1) * LANES]
            line = jnp.sum(spread_query * decayed[g, s], axis=0, keepdims=True)
            mixed[s : s + 1, g * LANES : (g + 1) * LANES] = line
    match = jnp.sum(query * keys, axis=1, keepdims=True)
    mark("out_dot_s2")
    fetched(8)
    arrived(12, ow.at[pl.ds(0, LANES), :], None)
    readout = (mixed[...] + match * values_f) * KEYS ** (-0.5)
    attn_part = dot(readout.astype(BF16), ow[...]).astype(BF16)
    for i in range(N // 2):
        sp[i] = attn_part[:, i * 2 * PIECE : (i + 1) * 2 * PIECE]
    for d in FAR:
        send(2, sp.at[lax.rem(z + d, N // 2)], rp.at[z], tp=tp_at(d, 0))
    sent(2, rp, N // 2 - 1)
    rp[z] = sp[z]
    for copy in own_weights:
        copy.start()
    for i, (mine, theirs) in enumerate(expert_weights(1 - c)):
        send(min(13 + i, 15), mine, theirs, tp=partner)

    mark("update")
    update = dot(jnp.transpose(keys).astype(BF16), values_wide)
    for g in range(2):
        for s in range(PART):
            at = (g * PART + s) * LANES
            decayed[g, s] = decayed[g, s] + update[:, at : at + LANES]
    mark("slots")
    fetched(9, 10, 11)
    slots = N * CAP
    routed = rt[...]
    ids = iota((N, ROWS), 0)
    chosen = ((routed[0:1, :] == ids) | (routed[1:2, :] == ids)).astype(F32)
    upper = (iota((ROWS, ROWS), 0) < iota((ROWS, ROWS), 1)).astype(BF16)
    rank = dot(chosen.astype(BF16), upper)
    expand = (iota((slots, N), 0) // CAP == iota((slots, N), 1)).astype(BF16)
    here = dot(expand, chosen.astype(BF16)) > 0.5
    place = dot(expand, rank.astype(BF16))
    spread = (here & (place == lax.rem(iota((slots, ROWS), 0), CAP).astype(F32))).astype(F32)

    mark("r2_wait")
    arrived(2, rp, N // 2 - 1)
    mark("s3_send")
    rg[t] = jnp.sum(rp[...].astype(F32), axis=0).astype(BF16)
    for p in ALL_TP:
        send(3, rg.at[t], rg.at[t], tp=tp_at(*p))
    sent(3, rg, N - 1)
    send(10, decayed.at[1 - c], ns_in, tp=partner)
    sent(10, ns_in, None)
    for s in range(PART):
        ns[c * PART + s] = decayed[c, s]
    mark("r3_wait")
    arrived(3, rg, N - 1)

    mark("norm1")
    def block(j, core):
        return pl.ds(pl.multiple_of((2 * j + core) * PIECE, PIECE), PIECE)

    for i in range(N // 2):
        cols = slice(i * 2 * PIECE, (i + 1) * 2 * PIECE)
        attn = jnp.concatenate([rg[2 * i].astype(F32), rg[2 * i + 1].astype(F32)], axis=0)
        hid[:, cols] = ALPHA * tok[:, cols].astype(F32) + attn
    hidden = hid[...]
    centred = hidden - jnp.mean(hidden, axis=1, keepdims=True)
    var = jnp.mean(centred * centred, axis=1, keepdims=True)
    nrm[...] = (centred * lax.rsqrt(var + EPSILON) * ng[...]).astype(BF16)

    mark("s4_send")
    half = jnp.concatenate([nrm[:, block(j, c)] for j in range(N // 2)], axis=1)
    sd[...] = dot(spread.astype(BF16), half).astype(BF16).reshape(N, CAP, HALF)
    for p in ALL_EP:
        to = ep_at(*p)
        send(4, sd.at[to], rd.at[e], ep=to)
    sent(4, sd, N - 1)
    rd[e] = sd[e]

    mark("gates")
    logits = dot_nt(rw[...], nrm[...])
    arrived(10, ns_in, None)
    for s in range(PART):
        ns[(1 - c) * PART + s] = ns_in[s]

    mark("r4_wait_fwd")
    arrived(4, rd, N - 1)
    mark("up")
    rows = rd[...].reshape(N * CAP, HALF)
    for copy in own_weights[:2]:
        copy.wait()
    arrived(13, gl.at[:, :, pl.ds(0, LANES)], None)
    arrived(14, gl.at[:, :, pl.ds(0, LANES)], None)
    su[...] = dot(rows, gl[...].reshape(HALF, 4 * LANES))
    send(5, su, ru, tp=partner)
    sent(5, su, None)
    mark("up_wait")
    arrived(5, ru, None)
    mark("down")
    pre_act = su[...] + ru[...]
    glu = jnp.minimum(pre_act[:, : 2 * LANES], LIMIT)
    linear = jnp.clip(pre_act[:, 2 * LANES :], -LIMIT, LIMIT)
    act = (glu * jax.nn.sigmoid(SLOPE * glu) * (linear + 1.0)).astype(BF16)

    mark("down")
    for copy in own_weights[2:]:
        copy.wait()
    arrived(15, dn.at[:, pl.ds(0, LANES), :], None)
    for j in range(N // 2):
        sr[:, :, j * PIECE : (j + 1) * PIECE] = dot(act, dn[j]).astype(BF16).reshape(N, CAP, PIECE)
    mark("s6_send")
    for p in ALL_EP:
        to = ep_at(*p)
        send(8, sr.at[to], rr.at[e], ep=to)
    sent(8, sr, N - 1)
    rr[e] = sr[e]
    mark("gates2")
    raised = jnp.where(chosen > 0.5, jnp.exp(logits), 0.0)
    gates = raised / jnp.sum(raised, axis=0, keepdims=True)
    gate_rows = spread * jnp.dot(
        expand.astype(F32), gates, precision=lax.Precision.HIGHEST, preferred_element_type=F32
    )
    gate_cols = jnp.transpose(gate_rows)
    gate_hi = gate_cols.astype(BF16)
    gate_lo = (gate_cols - gate_hi.astype(F32)).astype(BF16)

    mark("r6_wait")
    arrived(8, rr, N - 1)

    mark("mix_s7")
    back = rr[...].reshape(N * CAP, HALF)
    mix = (dot(gate_hi, back) + dot(gate_lo, back)).astype(BF16)
    for j in range(N // 2):
        sm[j] = mix[:, j * PIECE : (j + 1) * PIECE]
    for d in FAR:
        to = lax.rem(z + d, N // 2)
        send(9, sm.at[to], rm.at[z], tp=2 * to + c)
    sent(9, sm, N // 2 - 1)
    rm[z] = sm[z]
    mark("r7_wait")
    arrived(9, rm, N // 2 - 1)
    mark("stats_s8")
    own = nrm[:, pl.ds(pl.multiple_of(t * PIECE, PIECE), PIECE)].astype(F32)
    u = ALPHA * own + jnp.sum(rm[...].astype(F32), axis=0)

    ss[...] = moments(u)
    for p in ALL_TP:
        send(6, ss, rs.at[t], tp=tp_at(*p))
    sent(6, rs, N - 1)
    rs[t] = ss[...]
    mark("r8_wait")
    fetched(12)
    arrived(6, rs, N - 1)
    mark("final")
    mean, scale = merged(rs)
    out_ref[...] = ((u - mean) * scale * fg[...]).astype(BF16)

    mark("drain")
    sent(11, st.at[0], None)
    sent(12, ow.at[pl.ds(0, LANES), :], None)
    sent(13, gl.at[:, :, pl.ds(0, LANES)], None)
    sent(14, gl.at[:, :, pl.ds(0, LANES)], None)
    sent(15, dn.at[:, pl.ds(0, LANES), :], None)
    for phase, like, count in pending:
        whole(phase, like, count).wait_send()
    mark(None)


def written_out(out, state, out_h, state_h, sems):
    rows = [pl.ds(2 * i, 2) for i in range(ROWS // 2)]
    copies = [pltpu.make_async_copy(state.at[r], state_h.at[r], sems.at[i]) for i, r in enumerate(rows)]
    copies.append(pltpu.make_async_copy(out, out_h, sems.at[ROWS // 2]))
    for copy in copies:
        copy.start()
    for copy in copies:
        copy.wait()


def step(
    tokens, query_weight, key_weight, value_weight, decay_down, decay_up, decay_bias, old_state, out_weight,
    norm_gain, router_weight, routing, glu_weight, linear_weight, down_weight, final_gain,
):
    hbm = pl.BlockSpec(memory_space=pl.ANY)

    def in_blocks(weight):
        return weight.reshape(N // 2, 2, PIECE, LANES)

    vmem, dma = pltpu.VMEM, pltpu.SemaphoreType.DMA
    results = pl.pallas_call(
        kernel,
        out_shape=(
            pltpu.VMEM((ROWS, PIECE), BF16),
            pltpu.VMEM(old_state.shape, F32),
        ),
        in_specs=[hbm] * 16,
        out_specs=(pl.BlockSpec(memory_space=pltpu.VMEM), pl.BlockSpec(memory_space=pltpu.VMEM)),
        scratch_shapes=[
            vmem((ROWS, D), BF16), vmem((PIECE, 1024), BF16), vmem((PIECE, 1024), BF16), vmem((D, LANES), BF16),
            vmem((N, D), BF16), vmem((16, KEYS), F32), vmem((1, KEYS), F32), vmem((2, PART, KEYS, LANES), F32),
            vmem((2 * LANES, D), BF16), vmem((1, D), F32), vmem((N, D), BF16), vmem((2, ROWS), jnp.int32),
            vmem((N // 2, PIECE, 4 * LANES), BF16), vmem((N // 2, 2 * LANES, PIECE), BF16), vmem((1, PIECE), F32), vmem((PART, D), BF16), vmem((2, PART, KEYS, LANES), F32),
            vmem((2, 4, PART, 2 * KEYS), BF16), vmem((N, PART, 2 * KEYS), BF16), vmem((2, PART, LANES), F32),
            vmem((PART, LANES), F32), vmem((PART, 2 * LANES), F32), vmem((N // 2, PART, 2 * PIECE), BF16),
            vmem((N // 2, PART, 2 * PIECE), BF16), vmem((N, PART, 2 * PIECE), BF16), vmem((ROWS, D), F32), vmem((ROWS, D), BF16),
            vmem((N, CAP, HALF), BF16), vmem((N, CAP, HALF), BF16),
            vmem((N * CAP, 4 * LANES), F32), vmem((N * CAP, 4 * LANES), F32),
            vmem((N, CAP, HALF), BF16), vmem((N, CAP, HALF), BF16), vmem((N // 2, ROWS, PIECE), BF16),
            vmem((N // 2, ROWS, PIECE), BF16), vmem((1, LANES), F32), vmem((N, 1, LANES), F32), vmem((PART, KEYS, LANES), F32),
            dma((24,)), dma((16,)), dma((16,)),
        ],
        compiler_params=pltpu.CompilerParams(
            collective_id=0, has_side_effects=True, vmem_limit_bytes=60 * 1024 * 1024
        ),
        name="decode_step",
    )(
        tokens, query_weight, key_weight, value_weight, decay_down.T, decay_up, decay_bias.reshape(1, -1), old_state,
        out_weight, norm_gain.reshape(1, -1), router_weight.T, routing.T, in_blocks(glu_weight), in_blocks(linear_weight), down_weight,
        final_gain.reshape(1, -1),
    )
    results = [pltpu.with_memory_space_constraint(r, pltpu.VMEM) for r in results]
    return pl.pallas_call(
        written_out,
        out_shape=tuple(jax.ShapeDtypeStruct(r.shape, r.dtype) for r in results),
        in_specs=[pl.BlockSpec(memory_space=pltpu.VMEM)] * 2,
        out_specs=(hbm, hbm),
        scratch_shapes=[dma((ROWS // 2 + 1,))],
        name="written_out",
    )(*results)


def solution(mesh):
    in_specs = (
        P("ep", None), P("tp", None), P("tp", None), P(None, "tp"), P(), P(), P(), P("ep", None, "tp"), P("tp", None),
        P(), P(), P("ep", None), P("ep", None, "tp"), P("ep", None, "tp"), P("ep", "tp", None), P(),
    )
    out_specs = (P("ep", "tp"), P("ep", None, "tp"))
    return jax.shard_map(step, mesh=mesh, in_specs=in_specs, out_specs=out_specs, check_vma=False)
```

```python
import functools

import jax
import jax.numpy as jnp
from jax import lax
from jax.experimental import pallas as pl
from jax.experimental.pallas import tpu as pltpu
from jax.sharding import PartitionSpec as P

ALPHA = 2.0**0.25
TAU = 16.0
LIMIT = 7.0
SLOPE = 1.702
EPSILON = 1e-05
MESH = pl.DeviceIdType.MESH
F32 = jnp.float32
BF16 = jnp.bfloat16

N = 16
ROWS = 16
D = 4096
PIECE = 256
HALF = 2048
CAP = 4
PART = 8
KEYS = 256
LANES = 128
FAR = (4, 3, 5, 2, 6, 1, 7)
QUARTER = 1024
ALL_TP = [(d, x) for d in FAR for x in (1, 0)] + [(0, 1)]
ALL_EP = sorted(
    [(dy, dx) for dy in range(4) for dx in range(4) if dy or dx],
    key=lambda p: -sum(min(d, 4 - d) for d in p),
)


def dot(a, b):
    return jnp.dot(a, b, preferred_element_type=F32)


def dot_nt(a, b, precision=None):
    return lax.dot_general(a, b, (((1,), (1,)), ((), ())), precision=precision, preferred_element_type=F32)


def iota(shape, dim):
    return lax.broadcasted_iota(jnp.int32, shape, dim)


_scopes = []


def mark(name):
    while _scopes:
        _scopes.pop().__exit__(None, None, None)
    if name:
        _scopes.append(jax.named_scope(name))
        _scopes[-1].__enter__()


def remote(src, dst, send_sem, recv_sem, **where):
    return pltpu.make_async_remote_copy(
        src_ref=src, dst_ref=dst, send_sem=send_sem, recv_sem=recv_sem, device_id=where, device_id_type=MESH
    )


def thirds_of(x):
    high = x.astype(BF16).astype(F32)
    middle = (x - high).astype(BF16).astype(F32)
    return [high, middle, (x - high - middle).astype(BF16).astype(F32)]


def diagonal(offset):
    return iota((ROWS, LANES), 1) == iota((ROWS, LANES), 0) + offset


def moments(part):
    mean = jnp.mean(part, axis=1, keepdims=True)
    squares = jnp.sum((part - mean) ** 2, axis=1, keepdims=True)
    line = jnp.where(diagonal(0), mean, jnp.where(diagonal(ROWS), squares, 0.0))
    return jnp.sum(line, axis=0, keepdims=True)


def merged(lines):
    lines = jnp.concatenate([lines[i] for i in range(N)], axis=0)
    total = jnp.sum(lines, axis=0, keepdims=True)
    apart = jnp.sum((lines - total / N) ** 2, axis=0, keepdims=True)

    def column(line, offset):
        return jnp.sum(jnp.where(diagonal(offset), line, 0.0), axis=1, keepdims=True)

    variance = (column(total, ROWS) + PIECE * column(apart, 0)) / D
    return column(total / N, 0), lax.rsqrt(variance + EPSILON)


def kernel(
    tok_h, qw_h, kw_h, vw_h, dd_h, du_h, db_h, st_h, ow_h, ng_h, rw_h, rt_h, glu_h, lin_h, dn_h, fg_h,
    out_ref, ns,
    tok, qw, kw, vw, dd, du, db, st, ow, ng, rw, rt, gl, dn, fg, tok_part, decayed,
    sq, rq, vals, val_out, mixed, sp, rp, sg, rg, hid, nrm, sd, rd, su, sb, rb, sr, rr, sm, rm, ss, rs, ns_in, lg,
    loc, out_sem, in_sem,
):
    e = lax.axis_index("ep")
    t = lax.axis_index("tp")
    z = t // 2
    c = lax.rem(t, 2)
    head = t // 4
    partner = t + 1 - 2 * c

    def tp_at(d, x):
        return 2 * lax.rem(z + d, N // 2) + lax.rem(c + x, 2)

    def ep_at(dy, dx):
        return 4 * lax.rem(e // 4 + dy, 4) + lax.rem(lax.rem(e, 4) + dx, 4)

    def wide_piece(i):
        return pl.ds(pl.multiple_of(i * 2 * PIECE, 2 * PIECE), 2 * PIECE)

    def block(j, core):
        return pl.ds(pl.multiple_of((2 * j + core) * PIECE, PIECE), PIECE)

    mark("fetch")
    units = pl.ds(pl.multiple_of(c * LANES, LANES), LANES)
    linear_units = pl.ds(pl.multiple_of((2 + c) * LANES, LANES), LANES)

    def rows_of(core):
        return pl.ds(pl.multiple_of(core * PART, PART), PART)

    head_cols = pl.ds(pl.multiple_of(head * KEYS, KEYS), KEYS)
    fetches = [
        (tok_h, tok), (qw_h, qw), (kw_h, kw), (dd_h, dd), (du_h.at[:, head_cols], du), (db_h.at[:, head_cols], db),
        (vw_h, vw), (st_h.at[rows_of(c)], st.at[c]), (tok_h.at[rows_of(c), :], tok_part), (ow_h, ow.at[units, :]),
    ]
    copies = [pltpu.make_async_copy(a, b, loc.at[i]) for i, (a, b) in enumerate(fetches)]
    for copy in copies:
        copy.start()
    own_cols = pl.ds(pl.multiple_of(t * PIECE, PIECE), PIECE)
    later = [(ng_h, ng), (rw_h, rw), (rt_h, rt), (fg_h.at[:, own_cols], fg)]
    late_copies = [pltpu.make_async_copy(a, b, loc.at[3 + i]) for i, (a, b) in enumerate(later)]


    def expert_weights(core):
        return [
            (glu_h.at[:, core], gl.at[:, :, units]),
            (lin_h.at[:, core], gl.at[:, :, linear_units]),
            (dn_h.at[0], dn.at[units, :]),
        ]

    own_weights = [pltpu.make_async_copy(a, b, loc.at[i]) for i, (a, b) in enumerate(expert_weights(c))]

    def fetched(*which):
        for i in which:
            copies[i].wait()

    mark("barrier_signal")
    barrier = pltpu.get_barrier_semaphore()
    for p in ALL_TP:
        pl.semaphore_signal(barrier, inc=1, device_id={"tp": tp_at(*p)}, device_id_type=MESH)
    for p in ALL_EP:
        pl.semaphore_signal(barrier, inc=1, device_id={"ep": ep_at(*p)}, device_id_type=MESH)

    mark("qk_fetch_wait")
    fetched(0, 1, 2)
    mark("qk_dot")
    share = tok[:, pl.ds(pl.multiple_of(t * PIECE, PIECE), PIECE)]
    q_part = dot(share, qw[...]).astype(BF16)
    k_part = dot(share, kw[...]).astype(BF16)
    for i in range(4):
        cols = slice(i * KEYS, (i + 1) * KEYS)
        both = jnp.concatenate([q_part[:, cols], k_part[:, cols]], axis=1)
        sq[0, i] = both[:PART]
        sq[1, i] = both[PART:]
    mark("barrier_wait")
    pl.semaphore_wait(barrier, 2 * (N - 1))
    mark("s1_send")
    pending = []

    def send(phase, src, dst, **where):
        remote(src, dst, out_sem.at[phase], in_sem.at[phase], **where).start()

    def sent(phase, like, count):
        pending.append((phase, like, count))

    def whole(phase, like, count):
        ref = like if count is None else like.at[pl.ds(0, count)]
        return remote(ref, ref, out_sem.at[phase], in_sem.at[phase], tp=partner)

    def arrived(phase, like, count):
        whole(phase, like, count).wait_recv()

    for d, x in ALL_TP:
        to = tp_at(d, x)
        send(0, sq.at[lax.rem(to, 2), to // 4], rq.at[t], tp=to)
    sent(0, rq, N - 1)
    send(11, st_h.at[rows_of(1 - c)], st.at[c], tp=partner)
    send(12, ow_h, ow.at[units, :], tp=partner)
    rq[t] = sq[c, head]

    mark("decay")
    fetched(3, 4, 5, 6, 8)
    for copy in late_copies:
        copy.start()
    values = dot(tok[...], vw[...]).astype(BF16).astype(F32)
    mine_first = c == 0
    val_out[...] = jnp.where(mine_first, values[PART:], values[:PART])
    vals[c] = jnp.where(mine_first, values[:PART], values[PART:])
    send(1, val_out, vals.at[c], tp=partner)
    sent(1, val_out, None)
    low_rank = dot_nt(tok_part[...], dd[...])
    pre = jnp.dot(low_rank, du[...], precision=lax.Precision.HIGHEST, preferred_element_type=F32) + db[...]
    log_sig = -(jnp.maximum(-pre, 0.0) + jnp.log1p(jnp.exp(-jnp.abs(pre))))
    decay = jnp.exp(log_sig / TAU)
    thirds = jnp.concatenate(thirds_of(decay), axis=0)
    wide = PART * LANES
    ones3 = (lax.rem(iota((3 * PART, wide), 0), PART) == iota((3 * PART, wide), 1) // LANES).astype(BF16)
    decay_wide = dot(jnp.transpose(thirds).astype(BF16), ones3)
    mark("state_decay")
    fetched(7)
    arrived(11, st.at[0], None)
    for g in range(2):
        for s in range(PART):
            decayed[g, s] = decay_wide[:, s * LANES : (s + 1) * LANES] * st[g, s]
    own_block = iota((PART, wide), 0) == iota((PART, wide), 1) // LANES
    ones1 = own_block.astype(BF16)
    arrived(1, val_out, None)
    values_f = jnp.concatenate([vals[0], vals[1]], axis=1)
    values_wide = jnp.concatenate(
        [jnp.where(own_block, jnp.concatenate([vals[g]] * PART, axis=1), 0.0).astype(BF16) for g in range(2)], axis=1
    )
    mark("r1_wait")
    arrived(0, rq, N - 1)
    mark("state")
    query_keys = jnp.sum(rq[...].astype(F32), axis=0).astype(BF16).astype(F32)
    query, keys = query_keys[:, :KEYS], query_keys[:, KEYS:]
    query_wide = dot(jnp.transpose(query).astype(BF16), ones1)
    for g in range(2):
        for s in range(PART):
            spread_query = query_wide[:, s * LANES : (s + 1) * LANES]
            line = jnp.sum(spread_query * decayed[g, s], axis=0, keepdims=True)
            mixed[s : s + 1, g * LANES : (g + 1) * LANES] = line
    match = jnp.sum(query * keys, axis=1, keepdims=True)
    mark("out_dot_s2")
    fetched(9)
    arrived(12, ow.at[pl.ds(0, LANES), :], None)
    readout = (mixed[...] + match * values_f) * KEYS ** (-0.5)
    readout = readout.astype(BF16)
    for steps in ((4,), (3, 5), (2, 6), (1, 7)):
        for d in steps:
            to = lax.rem(z + d, N // 2)
            sp[to] = dot(readout, ow[:, wide_piece(to)]).astype(BF16)
        for d in steps:
            send(2, sp.at[lax.rem(z + d, N // 2)], rp.at[z], tp=tp_at(d, 0))
    sent(2, rp, N // 2 - 1)
    rp[z] = dot(readout, ow[:, wide_piece(z)]).astype(BF16)
    for copy in own_weights:
        copy.start()
    for i, (mine, theirs) in enumerate(expert_weights(1 - c)):
        send(13 + i, mine, theirs, tp=partner)

    mark("update")
    update = dot(jnp.transpose(keys).astype(BF16), values_wide)
    for g in range(2):
        for s in range(PART):
            at = (g * PART + s) * LANES
            decayed[g, s] = decayed[g, s] + update[:, at : at + LANES]
    mark("slots")
    for copy in late_copies:
        copy.wait()
    slots = N * CAP
    routed = rt[...]
    ids = iota((N, ROWS), 0)
    chosen = ((routed[0:1, :] == ids) | (routed[1:2, :] == ids)).astype(F32)
    upper = (iota((ROWS, ROWS), 0) < iota((ROWS, ROWS), 1)).astype(BF16)
    rank = dot(chosen.astype(BF16), upper)
    expand = (iota((slots, N), 0) // CAP == iota((slots, N), 1)).astype(BF16)
    here = dot(expand, chosen.astype(BF16)) > 0.5
    place = dot(expand, rank.astype(BF16))
    spread = (here & (place == lax.rem(iota((slots, ROWS), 0), CAP).astype(F32))).astype(F32)

    mark("r2_wait")
    arrived(2, rp, N // 2 - 1)
    mark("s3_send")
    attn = jnp.sum(rp[...].astype(F32), axis=0).astype(BF16)
    piece = ALPHA * tok_part[:, wide_piece(z)].astype(F32) + attn.astype(F32)
    part_mean = jnp.mean(piece, axis=1, keepdims=True)
    part_sq = jnp.sum((piece - part_mean) ** 2, axis=1, keepdims=True)
    lane = iota((PART, LANES), 1)
    stats = jnp.zeros((PART, LANES), F32)
    for i, third in enumerate(thirds_of(part_mean) + thirds_of(part_sq)):
        stats = jnp.where(lane == i, third, stats)
    for i in range(2):
        sg[i, :, :PIECE] = attn[:, i * PIECE : (i + 1) * PIECE]
        sg[i, :, PIECE:] = stats.astype(BF16)
    for d, x in ALL_TP:
        to = tp_at(d, x)
        send(3, sg.at[lax.rem(to, 2)], rg.at[t], tp=to)
    rg[t] = sg[c]
    sent(3, rg, N - 1)
    send(10, decayed.at[1 - c], ns_in, tp=partner)
    sent(10, ns_in, None)
    for s in range(PART):
        ns[c * PART + s] = decayed[c, s]
    rw_half = jnp.concatenate([rw[:, block(j, c)] for j in range(N // 2)], axis=1)
    ng_half = jnp.concatenate([ng[:, block(j, c)] for j in range(N // 2)], axis=1)
    for j in range(N // 2):
        hid[:, j * PIECE : (j + 1) * PIECE] = ALPHA * tok[:, block(j, c)].astype(F32)
    mark("r3_wait")
    arrived(3, rg, N - 1)

    mark("norm1")
    stats = rg[:, :, PIECE:].reshape(N * PART, LANES).astype(F32)
    lane = iota((N * PART, LANES), 1)

    def by_chip(first):
        column = jnp.sum(jnp.where((lane >= first) & (lane < first + 3), stats, 0.0), axis=1, keepdims=True)
        return [column[i * ROWS : (i + 1) * ROWS] for i in range(N // 2)]

    means, squares = by_chip(0), by_chip(3)
    mean = sum(means) / (N // 2)
    var = (sum(squares) + 2 * PIECE * sum((m - mean) ** 2 for m in means)) / D
    scale = lax.rsqrt(var + EPSILON)
    picked = spread.astype(BF16)
    for a in range(2):
        for j in range(4 * a, 4 * a + 4):
            cols = slice(j * PIECE, (j + 1) * PIECE)
            attn = jnp.concatenate([rg[2 * j, :, :PIECE].astype(F32), rg[2 * j + 1, :, :PIECE].astype(F32)], axis=0)
            nrm[:, cols] = ((hid[:, cols] + attn - mean) * scale * ng_half[:, cols]).astype(BF16)

        sd[a] = dot(picked, nrm[:, a * QUARTER : (a + 1) * QUARTER]).astype(BF16).reshape(N, CAP, QUARTER)
        for p in ALL_EP:
            to = ep_at(*p)
            send(4 + 12 * a, sd.at[a, to], rd.at[a, e], ep=to)
        sent(4 + 12 * a, sd.at[0], N - 1)
        rd[a, e] = sd[a, e]

    mark("gates")
    logit_part = dot_nt(rw_half, nrm[...])
    lg[c] = jnp.concatenate([logit_part, jnp.zeros((N, LANES - ROWS), F32)], axis=1)
    send(7, lg.at[c], lg.at[c], tp=partner)
    sent(7, lg, 1)
    arrived(10, ns_in, None)
    for s in range(PART):
        ns[(1 - c) * PART + s] = ns_in[s]

    mark("r4_wait_fwd")
    arrived(4, rd.at[0], N - 1)
    mark("up")
    for copy in own_weights[:2]:
        copy.wait()
    arrived(13, gl.at[:, :, pl.ds(0, LANES)], None)
    arrived(14, gl.at[:, :, pl.ds(0, LANES)], None)
    first = dot(rd[0].reshape(N * CAP, QUARTER), gl[0:4].reshape(QUARTER, 4 * LANES))
    mark("r4_wait2")
    arrived(16, rd.at[1], N - 1)
    mark("up2")
    su[...] = first + dot(rd[1].reshape(N * CAP, QUARTER), gl[4:8].reshape(QUARTER, 4 * LANES))
    sb[...] = su[...].astype(BF16)
    send(5, sb, rb, tp=partner)
    sent(5, sb, None)
    mark("up_wait")
    arrived(5, rb, None)
    mark("down")
    pre_act = su[...] + rb[...].astype(F32)
    glu = jnp.minimum(pre_act[:, : 2 * LANES], LIMIT)
    linear = jnp.clip(pre_act[:, 2 * LANES :], -LIMIT, LIMIT)
    act = (glu * jax.nn.sigmoid(SLOPE * glu) * (linear + 1.0)).astype(BF16)

    mark("down")
    own_weights[2].wait()
    arrived(15, dn.at[pl.ds(0, LANES), :], None)
    order = FAR + (0,)
    for a in range(2):
        for i in range(4):
            weights = dn[:, block(lax.rem(z + order[4 * a + i], N // 2), c)]
            sr[a, :, :, i * PIECE : (i + 1) * PIECE] = dot(act, weights).astype(BF16).reshape(N, CAP, PIECE)
        for p in ALL_EP:
            to = ep_at(*p)
            send(8 + 9 * a, sr.at[a, to], rr.at[a, e], ep=to)
        sent(8 + 9 * a, sr.at[0], N - 1)
        rr[a, e] = sr[a, e]
    mark("gates2")
    arrived(7, lg, 1)
    logits = (lg[0] + lg[1])[:, :ROWS]
    raised = jnp.where(chosen > 0.5, jnp.exp(logits), 0.0)
    gates = raised / jnp.sum(raised, axis=0, keepdims=True)
    gate_rows = spread * jnp.dot(
        expand.astype(F32), gates, precision=lax.Precision.HIGHEST, preferred_element_type=F32
    )
    gate_cols = jnp.transpose(gate_rows)
    gate_hi = gate_cols.astype(BF16)
    gate_lo = (gate_cols - gate_hi.astype(F32)).astype(BF16)

    mark("r6_wait")
    arrived(8, rr.at[0], N - 1)

    mark("mix_s7")
    def mixed_piece(i):
        back = rr[i // 4, :, :, (i % 4) * PIECE : (i % 4 + 1) * PIECE].reshape(N * CAP, PIECE)
        return (dot(gate_hi, back) + dot(gate_lo, back)).astype(BF16)

    for places in ((0,), (1, 2, 3), (4, 5, 6)):
        if places[0] == 4:
            mark("r6_wait2")
            arrived(17, rr.at[1], N - 1)
            mark("mix2")
        for i in places:
            sm[lax.rem(z + order[i], N // 2)] = mixed_piece(i)
        for i in places:
            to = lax.rem(z + order[i], N // 2)
            send(9, sm.at[to], rm.at[z], tp=2 * to + c)
    sent(9, sm, N // 2 - 1)
    rm[z] = mixed_piece(7)
    mark("r7_wait")
    arrived(9, rm, N // 2 - 1)
    mark("stats_s8")
    own = nrm[:, pl.ds(pl.multiple_of(z * PIECE, PIECE), PIECE)].astype(F32)
    u = ALPHA * own + jnp.sum(rm[...].astype(F32), axis=0)

    ss[...] = moments(u)
    for p in ALL_TP:
        send(6, ss, rs.at[t], tp=tp_at(*p))
    sent(6, rs, N - 1)
    rs[t] = ss[...]
    mark("r8_wait")
    arrived(6, rs, N - 1)
    mark("final")
    mean, scale = merged(rs)
    out_ref[...] = ((u - mean) * scale * fg[...]).astype(BF16)

    mark("drain")
    sent(11, st.at[0], None)
    sent(12, ow.at[pl.ds(0, LANES), :], None)
    sent(13, gl.at[:, :, pl.ds(0, LANES)], None)
    sent(14, gl.at[:, :, pl.ds(0, LANES)], None)
    sent(15, dn.at[pl.ds(0, LANES), :], None)
    for phase, like, count in pending:
        whole(phase, like, count).wait_send()
    mark(None)


def written_out(out, state, out_h, state_h, sems):
    rows = [pl.ds(2 * i, 2) for i in range(ROWS // 2)]
    copies = [pltpu.make_async_copy(state.at[r], state_h.at[r], sems.at[i]) for i, r in enumerate(rows)]
    copies.append(pltpu.make_async_copy(out, out_h, sems.at[ROWS // 2]))
    for copy in copies:
        copy.start()
    for copy in copies:
        copy.wait()


def step(
    tokens, query_weight, key_weight, value_weight, decay_down, decay_up, decay_bias, old_state, out_weight,
    norm_gain, router_weight, routing, glu_weight, linear_weight, down_weight, final_gain,
):
    hbm = pl.BlockSpec(memory_space=pl.ANY)

    def in_blocks(weight):
        return weight.reshape(N // 2, 2, PIECE, LANES)

    vmem, dma = pltpu.VMEM, pltpu.SemaphoreType.DMA
    results = pl.pallas_call(
        kernel,
        out_shape=(
            pltpu.VMEM((ROWS, PIECE), BF16),
            pltpu.VMEM(old_state.shape, F32),
        ),
        in_specs=[hbm] * 16,
        out_specs=(pl.BlockSpec(memory_space=pltpu.VMEM), pl.BlockSpec(memory_space=pltpu.VMEM)),
        scratch_shapes=[
            vmem((ROWS, D), BF16), vmem((PIECE, 1024), BF16), vmem((PIECE, 1024), BF16), vmem((D, LANES), BF16),
            vmem((N, D), BF16), vmem((16, KEYS), F32), vmem((1, KEYS), F32), vmem((2, PART, KEYS, LANES), F32),
            vmem((2 * LANES, D), BF16), vmem((1, D), F32), vmem((N, D), BF16), vmem((2, ROWS), jnp.int32),
            vmem((N // 2, PIECE, 4 * LANES), BF16), vmem((2 * LANES, D), BF16), vmem((1, PIECE), F32), vmem((PART, D), BF16), vmem((2, PART, KEYS, LANES), F32),
            vmem((2, 4, PART, 2 * KEYS), BF16), vmem((N, PART, 2 * KEYS), BF16), vmem((2, PART, LANES), F32),
            vmem((PART, LANES), F32), vmem((PART, 2 * LANES), F32), vmem((N // 2, PART, 2 * PIECE), BF16),
            vmem((N // 2, PART, 2 * PIECE), BF16), vmem((2, PART, PIECE + LANES), BF16), vmem((N, PART, PIECE + LANES), BF16), vmem((ROWS, HALF), F32), vmem((ROWS, HALF), BF16),
            vmem((2, N, CAP, QUARTER), BF16), vmem((2, N, CAP, QUARTER), BF16),
            vmem((N * CAP, 4 * LANES), F32), vmem((N * CAP, 4 * LANES), BF16), vmem((N * CAP, 4 * LANES), BF16),
            vmem((2, N, CAP, QUARTER), BF16), vmem((2, N, CAP, QUARTER), BF16), vmem((N // 2, ROWS, PIECE), BF16),
            vmem((N // 2, ROWS, PIECE), BF16), vmem((1, LANES), F32), vmem((N, 1, LANES), F32), vmem((PART, KEYS, LANES), F32), vmem((2, N, LANES), F32),
            dma((10,)), dma((18,)), dma((18,)),
        ],
        compiler_params=pltpu.CompilerParams(
            collective_id=0, has_side_effects=True, vmem_limit_bytes=60 * 1024 * 1024
        ),
        name="decode_step",
    )(
        tokens, query_weight, key_weight, value_weight, decay_down.T, decay_up, decay_bias.reshape(1, -1), old_state,
        out_weight, norm_gain.reshape(1, -1), router_weight.T, routing.T, in_blocks(glu_weight), in_blocks(linear_weight), down_weight,
        final_gain.reshape(1, -1),
    )
    results = [pltpu.with_memory_space_constraint(r, pltpu.VMEM) for r in results]
    return pl.pallas_call(
        written_out,
        out_shape=tuple(jax.ShapeDtypeStruct(r.shape, r.dtype) for r in results),
        in_specs=[pl.BlockSpec(memory_space=pltpu.VMEM)] * 2,
        out_specs=(hbm, hbm),
        scratch_shapes=[dma((ROWS // 2 + 1,))],
        name="written_out",
    )(*results)


def solution(mesh):
    in_specs = (
        P("ep", None), P("tp", None), P("tp", None), P(None, "tp"), P(), P(), P(), P("ep", None, "tp"), P("tp", None),
        P(), P(), P("ep", None), P("ep", None, "tp"), P("ep", None, "tp"), P("ep", "tp", None), P(),
    )
    out_specs = (P("ep", "tp"), P("ep", None, "tp"))
    return jax.shard_map(step, mesh=mesh, in_specs=in_specs, out_specs=out_specs, check_vma=False)
```
